512 devices in a mesh: grp: 2 (over y), sp: 32 (over z, core), tp: 8 (over x).
Axes of the slice: x: 8, y: 2, z: 16, core: 2. Of those that a mesh axis runs over, the one named last changes fastest.
The devices are a block of a 8x8x16 slice.
Arguments:
- tokens_in: bfloat16 [16384, 2048], P(('grp', 'sp'), 'tp'), parts along dimension 0, may hold values from -6 to 6
- norm_gain: float32 [3, 2048], replicated, may hold values from 0.1 to 1.9
- w_pool_in: bfloat16 [3, 2048, 1024], P(None, 'sp', 'tp'), may hold values from -0.125 to 0.125
- w_gate: bfloat16 [3, 2048, 2048], P(None, 'sp', 'tp'), may hold values from -0.125 to 0.125
- w_back: bfloat16 [3, 1024, 2048], P(None, 'tp', 'sp'), may hold values from -0.375 to 0.375
Outputs:
- tokens_out: bfloat16 [16384, 2048], P(('grp', 'sp'), 'tp'), parts along dimension 0
The draws below stay inside these ranges and needn't reach their ends.
There are 2 independent parts, one for each index of `grp`. The reference program is written for one: setup_inputs(seed, part) draws one part's arguments, and reference() takes and returns one part's arrays. A program takes and returns all parts, laid end to end along the dimension named above; an argument that names none is the same for every part. Nothing has to cross between parts.
All inputs are finite; a program needn't handle non-finite values.
Results may differ from the reference program's by a relative error of at most 0.017.
Values may be sent and summed in bfloat16 or wider, within the bound.
A program may use at most 64 MiB of HBM per device.

```python
import jax
import jax.numpy as jnp
from jax import lax

D = 2048
POOL_WIDTH = 1024
GROUPS = 4
GRID_W = 32
LAYERS = 3
TOKENS = 8192
N_TP = 8


def spiked(drawn, key, source, target, blocks, factor):
    def block_of(axis_at):
        return (jnp.arange(drawn.shape[axis_at]) // (drawn.shape[axis_at] // blocks)).reshape((-1,) + (1,) * (drawn.ndim - 1 - axis_at))

    near = jax.random.permutation(key, blocks)[block_of(target)]
    second = (block_of(target) + blocks // 2) % blocks
    return jnp.where((block_of(source) == near) | (block_of(source) == second), factor * drawn, drawn)


def shard_levels(own_key, shape, shards, smallest, top_value):
    loudness = 1.0
    for axis_at, shards_of in shards:
        heights = jax.random.uniform(jax.random.fold_in(jax.random.fold_in(own_key, 6), axis_at), (shards_of,), jnp.float32, smallest / len(shards), top_value / len(shards))
        loudness = loudness * jnp.repeat(jnp.exp(heights), shape[axis_at] // shards_of).reshape((-1,) + (1,) * (len(shape) - 1 - axis_at))
    return loudness


def normal_values(rng, dims, deviation, most, cuts=(), kind=jnp.bfloat16):
    array = jax.random.normal(rng, dims, jnp.float32) * deviation
    if len(cuts) > 0:
        array = shard_levels(rng, dims, cuts, -0.22, 0.18) * array
    return jnp.clip(array, min=-most, max=most).astype(kind)


def heavy_noise(stream_key, extent, width, bound, cuts, heavy, kind=jnp.bfloat16):
    drawn = width * jax.random.normal(stream_key, extent, jnp.float32)
    if cuts:
        drawn = drawn * shard_levels(stream_key, extent, cuts, -0.22, 0.18)
    return jnp.clip(spiked(drawn, jax.random.fold_in(stream_key, 3), *heavy), -bound, bound).astype(kind)


def setup_inputs(seed: int = 0, part: int = 0) -> dict:
    arg_keys = jax.random.split(jax.random.key(seed), 6)
    part_splits = jax.random.split(jax.random.fold_in(arg_keys[5], part), 6)
    return {
        "tokens_in": normal_values(part_splits[0], (TOKENS, D), 1.0, 6.0, ((0, 32), (1, 8))),
        "norm_gain": jnp.clip(1.0 + 0.18 * jax.random.normal(arg_keys[1], (LAYERS, D), jnp.float32), 0.1, 1.9),
        "w_pool_in": normal_values(arg_keys[2], (LAYERS, D, POOL_WIDTH), D ** -0.5, 0.125, ((1, 32), (2, 8))),
        "w_gate": normal_values(arg_keys[3], (LAYERS, D, D), D ** -0.5, 0.125, ((1, 32), (2, 8))),
        "w_back": heavy_noise(arg_keys[4], (LAYERS, POOL_WIDTH, D), POOL_WIDTH ** -0.5, 0.375, ((1, 8), (2, 32)), (1, 2, 32, 2.75)),
    }


pool_windows = (2, 4, 8, 16)
norm_eps = 1e-06

def window_means(padded, rows_here, first_row, total_rows, window):
    reach = max(pool_windows) // 2
    half_span = window // 2
    width_cols = padded.shape[1] - 2 * reach
    row_sums = padded[reach - half_span:reach - half_span + rows_here]
    for offset in range(1 - half_span, half_span):
        row_sums = row_sums + padded[reach + offset:reach + offset + rows_here]
    box_sums = row_sums[:, reach - half_span:reach - half_span + width_cols]
    for offset in range(1 - half_span, half_span):
        box_sums = box_sums + row_sums[:, reach + offset:reach + offset + width_cols]
    row_index = first_row + jnp.arange(rows_here, dtype=jnp.int32)
    col_index = jnp.arange(width_cols, dtype=jnp.int32)
    row_counts = jnp.minimum(row_index + half_span, total_rows) - jnp.maximum(row_index - half_span, 0)
    col_counts = jnp.minimum(col_index + half_span, width_cols) - jnp.maximum(col_index - half_span, 0)
    counts = (row_counts[:, None] * col_counts[None, :]).astype(jnp.float32)
    return box_sums / counts[:, :, None]

def reference(tokens_in, norm_gain, w_pool_in, w_gate, w_back):
    reach = max(pool_windows) // 2
    group_width = POOL_WIDTH // GROUPS
    total_rows = TOKENS // GRID_W
    block_width = POOL_WIDTH // N_TP
    state = tokens_in
    for layer_id in range(LAYERS):
        wide = state.astype(jnp.float32)
        normed = (wide * lax.rsqrt(lax.optimization_barrier(jnp.mean(wide * wide, axis=-1, keepdims=True)) + norm_eps) * norm_gain[layer_id]).astype(jnp.bfloat16)
        pool_in = jnp.dot(normed, w_pool_in[layer_id], preferred_element_type=jnp.float32).astype(jnp.bfloat16)
        gate = jax.nn.sigmoid(jnp.dot(normed, w_gate[layer_id], preferred_element_type=jnp.float32))
        cells = pool_in.astype(jnp.float32).reshape(total_rows, GRID_W, POOL_WIDTH)
        padded = jnp.pad(cells, ((reach, reach), (reach, reach), (0, 0)))
        pieces = []
        for group_id in range(GROUPS):
            chosen = padded[:, :, group_id * group_width:(group_id + 1) * group_width]
            pieces.append(window_means(chosen, total_rows, 0, total_rows, pool_windows[group_id]))
        means = jnp.concatenate(pieces, axis=2)
        pooled = (means - cells).reshape(TOKENS, POOL_WIDTH).astype(jnp.bfloat16)
        branch = jnp.zeros((TOKENS, D), jnp.float32)
        for block_id in range(N_TP):
            lower = block_id * block_width
            partial_value = jnp.dot(pooled[:, lower:lower + block_width], w_back[layer_id][lower:lower + block_width], preferred_element_type=jnp.float32).astype(jnp.bfloat16)
            branch = branch + lax.optimization_barrier(partial_value).astype(jnp.float32)
        state = (wide + gate * branch).astype(jnp.bfloat16)
    return state
```

```python
import functools

import jax
import jax.numpy as jnp
from jax import lax
from jax.experimental import pallas as pl
from jax.experimental.pallas import tpu as pltpu
from jax.sharding import PartitionSpec as P

MESH = pl.DeviceIdType.MESH
F32 = jnp.float32
BF16 = jnp.bfloat16
GRID_W = 32
GROUPS = 4
EPS = 1e-6
CHUNKS = 2


def mixer(n_sp, n_tp, tok_ref, gain_ref, wpool_ref, wgate_ref, wback_ref, out_ref,
          xs, ps, xg, w_pg, w_b, pin, halo, boxm, inv_count, gate, sumsq, swap_src,
          x_recv, p_recv, a_recv, b_recv, halo_recv, peer_recv, swap_recv,
          x_send, p_send, a_send, b_send, peer_send, halo_send, swap_send):
    layers = gain_ref.shape[0]
    tokens, feat = tok_ref.shape
    chan = wpool_ref.shape[2]
    rows_w = wpool_ref.shape[1]
    ct = tokens // CHUNKS
    half_tp = n_tp // 2
    n_z = n_sp // 2
    half_z = n_z // 2
    q_n = n_sp // n_tp
    sp = lax.axis_index("sp")
    tp = lax.axis_index("tp")

    def tp_at(d):
        return lax.rem(tp + (d + n_tp), n_tp)

    def sp_at(d):
        return lax.rem(sp + (2 * d + n_sp), n_sp)

    peer = sp + 1 - 2 * lax.rem(sp, 2)
    before = lax.rem(sp + n_sp - 1, n_sp)
    after = lax.rem(sp + 1, n_sp)
    quad = lax.rem(sp, q_n)
    swap_to = (q_n * lax.rem(tp + half_tp, n_tp) + quad, sp // q_n)
    swap_from = (q_n * tp + quad, lax.rem(sp // q_n + half_tp, n_tp))

    barrier = pltpu.get_barrier_semaphore()
    greet = [{"tp": tp_at(1)}, {"tp": tp_at(-1)}, {"sp": before}, {"sp": after},
             {"sp": sp_at(1)}, {"sp": sp_at(-1)}, {"sp": sp_at(2)}, {"sp": sp_at(-2)},
             {"sp": swap_from[0], "tp": swap_from[1]}]
    for who in greet:
        pl.semaphore_signal(barrier, inc=1, device_id=who, device_id_type=MESH)

    own_rows = pl.ds(pl.multiple_of(sp * rows_w, rows_w), rows_w)
    for l in range(layers):
        w_pg[l, own_rows, 0:chan] = wpool_ref[l]
        w_pg[l, own_rows, chan:] = wgate_ref[l]
        swap_src[l] = wback_ref[l].astype(F32).T.astype(BF16)
    for c in range(CHUNKS):
        xs[0, c, tp] = tok_ref[c * ct:(c + 1) * ct, :]

    pl.semaphore_wait(barrier, len(greet))

    def start(src, dst, send, recv, who):
        pltpu.make_async_remote_copy(src_ref=src, dst_ref=dst, send_sem=send, recv_sem=recv,
                                     device_id=who, device_id_type=MESH).start()

    def arrived(ref, sem):
        pltpu.make_async_copy(ref, ref, sem).wait()

    def reach(way, c):
        if half_tp * 2 == n_tp and (c % 2 == 0) != (way == 0):
            return half_tp - 1
        return half_tp

    def x_start(buf, l, c, d, send, recv):
        for way in (0, 1):
            if d <= reach(way, c):
                x_start_way(buf, l, c, d, send, recv, way)

    def x_start_way(buf, l, c, d, send, recv, way):
        step = 1 if way == 0 else -1
        block = buf.at[l, c, tp_at(-step * (d - 1))]
        start(block, block, send.at[l], recv.at[l, way, d - 1, c], {"tp": tp_at(step)})

    def x_wait_way(buf, l, c, d, recv, way):
        step = 1 if way == 0 else -1
        arrived(buf.at[l, c, tp_at(-step * d)], recv.at[l, way, d - 1, c])

    def z_reach(way):
        return half_z if way == 0 else n_z - 1 - half_z

    def z_rows(d):
        return pl.ds(pl.multiple_of(sp_at(d) * rows_w, rows_w), rows_w)

    def z_send(buf, l, kind, d0, width, send, recv, way):
        step = 1 if way == 0 else -1
        piece = buf.at[l, z_rows(-step * d0)]
        for r in range(1, width + 1):
            if d0 + r <= z_reach(way):
                start(piece, piece, send.at[l], recv.at[l, way, d0 + r - 1], {"sp": sp_at(step * r)})

    def z_peer(buf, l, kind, d):
        piece = buf.at[l, z_rows(d)]
        start(piece, piece, peer_send.at[kind, l], peer_recv.at[kind, l], {"sp": peer})

    def z_begin(kind, l, width):
        buf, send, recv = z_parts(kind)
        for way in (0, 1):
            z_send(buf, l, kind, 0, width, send, recv, way)
        z_peer(buf, l, kind, 0)

    def z_parts(kind):
        return (w_pg, a_send, a_recv) if kind == 0 else (w_b, b_send, b_recv)

    def z_stage(kind, l, stage, width):
        buf, send, recv = z_parts(kind)
        for r in range(width, 0, -1):
            d = (stage - 1) * width + r
            for way in (0, 1):
                step = 1 if way == 0 else -1
                if d <= z_reach(way):
                    arrived(buf.at[l, z_rows(-step * d)], recv.at[l, way, d - 1])
                    if r == width:
                        z_send(buf, l, kind, d, width, send, recv, way)
                    z_peer(buf, l, kind, -step * d)

    def z_peers_done(kind, l):
        buf = z_parts(kind)[0]
        arrived(buf.at[l, pl.ds(0, n_z * rows_w)], peer_recv.at[kind, l])

    def prep(l, c, j):
        block = xs[l, c, j].astype(F32)
        lanes = pl.ds(pl.multiple_of(j * feat, feat), feat)
        squares = block * block
        part = squares[:, 0:128]
        for k in range(1, feat // 128):
            part = part + squares[:, k * 128:(k + 1) * 128]
        sumsq[c * ct:(c + 1) * ct, :] += part
        xg[c * ct:(c + 1) * ct, lanes] = (block * gain_ref[l, :, lanes]).astype(BF16)

    for c in range(CHUNKS):
        x_start(xs, 0, c, 1, x_send, x_recv)
        if c == 0:
            z_begin(0, 0, 2)
            start(swap_src, w_b.at[:, pl.ds(pl.multiple_of(swap_to[0] * rows_w, rows_w), rows_w)], swap_send, swap_recv,
                  {"sp": swap_to[0], "tp": swap_to[1]})

    window = lax.shift_left(2, (tp * chan) // (n_tp * chan // GROUPS))
    reach_w = window // 2
    grid_rows = tokens // GRID_W
    first = sp * grid_rows
    total = grid_rows * n_sp
    ti = lax.broadcasted_iota(jnp.int32, (tokens, tokens), 0)
    tj = lax.broadcasted_iota(jnp.int32, (tokens, tokens), 1)
    ri, ci = ti // GRID_W, ti % GRID_W
    cj = tj % GRID_W
    col_in = (cj >= ci - reach_w) & (cj < ci + reach_w)
    for k in range(3):
        rj = tj // GRID_W + (k - 1) * grid_rows
        inside = col_in & (rj >= ri - reach_w) & (rj < ri + reach_w)
        boxm[k] = jnp.where(inside, 1.0, 0.0).astype(BF16)
    tr = lax.broadcasted_iota(jnp.int32, (tokens, chan), 0)
    r_at, c_at = tr // GRID_W + first, tr % GRID_W
    r_n = jnp.minimum(r_at + reach_w, total) - jnp.maximum(r_at - reach_w, 0)
    c_n = jnp.minimum(c_at + reach_w, GRID_W) - jnp.maximum(c_at - reach_w, 0)
    inv_count[...] = 1.0 / (r_n * c_n).astype(F32)

    @pl.when(sp == 0)
    def _():
        for l in range(layers):
            halo[l, 0] = jnp.zeros((tokens, chan), BF16)

    @pl.when(sp == n_sp - 1)
    def _():
        for l in range(layers):
            halo[l, 1] = jnp.zeros((tokens, chan), BF16)

    for l in range(layers):
        sumsq[...] = jnp.zeros_like(sumsq)
        for c in range(CHUNKS):
            prep(l, c, tp)
        if l > 0:
            z_begin(1, l, 1)
        if l + 1 < layers and l > 0:
            z_begin(0, l + 1, 1)
        for d in range(1, half_tp + 1):
            for c in range(CHUNKS):
                for way in (0, 1):
                    if d <= reach(way, c):
                        x_wait_way(xs, l, c, d, x_recv, way)
                        if d + 1 <= reach(way, c):
                            x_start_way(xs, l, c, d + 1, x_send, x_recv, way)
                for way in (0, 1):
                    if d <= reach(way, c):
                        prep(l, c, tp_at(-d if way == 0 else d))
            if l == 0:
                z_stage(0, 0, d, 2)
            else:
                z_stage(0, l, half_tp + d, 1)
                z_stage(1, l, d, 1)
        z_peers_done(0, l)

        scale = lax.rsqrt(jnp.sum(sumsq[...], axis=1, keepdims=True) * (1.0 / (n_tp * feat)) + EPS)
        pool = jnp.dot(xg[...], w_pg[l, :, 0:chan], preferred_element_type=F32)
        pin[l] = (pool * scale).astype(BF16)

        @pl.when(sp > 0)
        def _():
            start(pin.at[l], halo.at[l, 1], halo_send.at[l, 1], halo_recv.at[l, 1], {"sp": before})

        @pl.when(sp < n_sp - 1)
        def _():
            start(pin.at[l], halo.at[l, 0], halo_send.at[l, 0], halo_recv.at[l, 0], {"sp": after})

        if l == 0:
            arrived(w_b.at[:, own_rows], swap_recv)
            z_begin(1, 0, 2)
        if l + 1 < layers and l == 0:
            z_begin(0, l + 1, 1)
        gate_acc = jnp.dot(xg[...], w_pg[l, :, chan:], preferred_element_type=F32)
        gate[...] = jax.nn.sigmoid(gate_acc * scale)
        own_pool = pin[l]
        box = jnp.dot(boxm[1], own_pool, preferred_element_type=F32)

        @pl.when(sp > 0)
        def _():
            arrived(halo.at[l, 0], halo_recv.at[l, 0])

        @pl.when(sp < n_sp - 1)
        def _():
            arrived(halo.at[l, 1], halo_recv.at[l, 1])

        box = box + jnp.dot(boxm[0], halo[l, 0], preferred_element_type=F32)
        box = box + jnp.dot(boxm[2], halo[l, 1], preferred_element_type=F32)
        pooled = (box * inv_count[...] - own_pool.astype(F32)).astype(BF16)
        for c in range(CHUNKS):
            ps[l, c, tp] = pooled[c * ct:(c + 1) * ct]
            x_start(ps, l, c, 1, p_send, p_recv)

        def finish(c):
            branch = None
            for p in range(n_tp):
                term = lax.dot_general(ps[l, c, (p + half_tp) % n_tp], w_b[l, p * feat:(p + 1) * feat],
                                       (((1,), (1,)), ((), ())), preferred_element_type=F32)
                branch = term if branch is None else branch + term
            rows = slice(c * ct, (c + 1) * ct)
            new = (xs[l, c, tp].astype(F32) + gate[rows] * branch).astype(BF16)
            if l + 1 < layers:
                xs[l + 1, c, tp] = new
                x_start(xs, l + 1, c, 1, x_send, x_recv)
            else:
                out_ref[rows, :] = new

        for d in range(1, half_tp + 1):
            if d == half_tp:
                if l == 0:
                    z_stage(1, 0, d, 2)
                else:
                    z_stage(1, l, half_tp + d, 1)
                if l + 1 < layers:
                    z_stage(0, l + 1, d, 1)
                z_peers_done(1, l)
            for c in range(CHUNKS):
                for way in (0, 1):
                    if d <= reach(way, c):
                        x_wait_way(ps, l, c, d, p_recv, way)
                        if d + 1 <= reach(way, c):
                            x_start_way(ps, l, c, d + 1, p_send, p_recv, way)
                if d == half_tp:
                    finish(c)
            if d < half_tp:
                if l == 0:
                    z_stage(1, 0, d, 2)
                else:
                    z_stage(1, l, half_tp + d, 1)
                if l + 1 < layers:
                    z_stage(0, l + 1, d, 1)

    x_sends = sum(reach(way, c) for way in (0, 1) for c in range(CHUNKS))
    z_sends = {}
    for width in (1, 2):
        z_sends[width] = sum(
            1 for way in (0, 1) for d0 in range(0, half_z, width) for r in range(1, width + 1)
            if d0 + r <= z_reach(way))
    arrived(swap_src, swap_send)

    def drained(sem, ref, count, size):
        while count:
            now = min(count, size)
            arrived(ref.at[pl.ds(0, now * (ref.shape[0] // size))], sem)
            count -= now

    for l in range(layers):
        for buf, send in ((xs, x_send), (ps, p_send)):
            arrived_many(buf, l, x_sends, send.at[l])
        for kind in (0, 1):
            buf, send, _ = z_parts(kind)
            width = 2 if l == 0 else 1
            drained(send.at[l], buf.at[l], z_sends[width], n_sp)
            drained(peer_send.at[kind, l], buf.at[l], n_z, n_sp)

        @pl.when(sp > 0)
        def _():
            arrived(pin.at[l], halo_send.at[l, 1])

        @pl.when(sp < n_sp - 1)
        def _():
            arrived(pin.at[l], halo_send.at[l, 0])


def arrived_many(buf, l, count, sem):
    per = buf.shape[2]
    c = 0
    while count:
        now = min(count, per)
        ref = buf.at[l, c % CHUNKS, pl.ds(0, now)]
        pltpu.make_async_copy(ref, ref, sem).wait()
        count -= now
        c += 1


def solution(mesh):
    n_sp, n_tp = mesh.shape["sp"], mesh.shape["tp"]

    def on_device(tokens_in, norm_gain, w_pool_in, w_gate, w_back):
        layers = norm_gain.shape[0]
        tokens, feat = tokens_in.shape
        rows_w, chan = w_pool_in.shape[1:]
        rows = n_sp * rows_w
        ct = tokens // CHUNKS
        half_tp = n_tp // 2
        half_z = n_sp // 4
        dma = pltpu.SemaphoreType.DMA
        vmem = pl.BlockSpec(memory_space=pltpu.VMEM)
        return pl.pallas_call(
            functools.partial(mixer, n_sp, n_tp),
            out_shape=jax.ShapeDtypeStruct((tokens, feat), BF16),
            in_specs=[vmem] * 5,
            out_specs=vmem,
            scratch_shapes=[
                pltpu.VMEM((layers, CHUNKS, n_tp, ct, feat), BF16),
                pltpu.VMEM((layers, CHUNKS, n_tp, ct, chan), BF16),
                pltpu.VMEM((tokens, n_tp * feat), BF16),
                pltpu.VMEM((layers, rows, chan + feat), BF16),
                pltpu.VMEM((layers, rows, chan), BF16),
                pltpu.VMEM((layers, tokens, chan), BF16),
                pltpu.VMEM((layers, 2, tokens, chan), BF16),
                pltpu.VMEM((3, tokens, tokens), BF16),
                pltpu.VMEM((tokens, chan), F32),
                pltpu.VMEM((tokens, feat), F32),
                pltpu.VMEM((tokens, 128), F32),
                pltpu.VMEM((layers, rows_w, chan), BF16),
                dma((layers, 2, half_tp, CHUNKS)),
                dma((layers, 2, half_tp, CHUNKS)),
                dma((layers, 2, half_z)),
                dma((layers, 2, half_z)),
                dma((layers, 2)),
                dma((2, layers)),
                dma,
                dma((layers,)),
                dma((layers,)),
                dma((layers,)),
                dma((layers,)),
                dma((2, layers)),
                dma((layers, 2)),
                dma,
            ],
            compiler_params=pltpu.CompilerParams(
                collective_id=0, has_side_effects=True, vmem_limit_bytes=48 * 1024 * 1024),
        )(tokens_in, norm_gain.reshape(layers, 1, -1), w_pool_in, w_gate, w_back)

    return jax.shard_map(
        on_device,
        mesh=mesh,
        in_specs=(
            P(("grp", "sp"), "tp"),
            P(),
            P(None, "sp", "tp"),
            P(None, "sp", "tp"),
            P(None, "tp", "sp"),
        ),
        out_specs=P(("grp", "sp"), "tp"),
        check_vma=False,
    )
```

```python
import functools

import jax
import jax.numpy as jnp
from jax import lax
from jax.experimental import pallas as pl
from jax.experimental.pallas import tpu as pltpu
from jax.sharding import PartitionSpec as P

MESH = pl.DeviceIdType.MESH
F32 = jnp.float32
BF16 = jnp.bfloat16
GRID_W = 32
GROUPS = 4
EPS = 1e-6
CHUNKS = 2
scope = jax.named_scope

RING = {1: 0, 2: 1, 3: 2, 4: 3}
PAIRS = {1: 0, 2: 0, 3: 2, 4: 2, 5: 4, 6: 4, 7: 6, 8: 6}
FOURS = {1: 0, 2: 0, 3: 0, 4: 0, 5: 4, 6: 4, 7: 4, 8: 4}
STATE_TREE = RING
POOLED_TREE = PAIRS
POOL_W, GATE_W, BACK_W = 0, 1, 2


def weight_tree(kind, l):
    if l == 0 or kind == BACK_W:
        return FOURS
    return PAIRS


def depth(tree, d):
    return 0 if d == 0 else 1 + depth(tree, tree[d])


def stages(tree, most):
    deep = max(depth(tree, d) for d in range(1, most + 1))
    return [sorted((d for d in range(1, most + 1) if depth(tree, d) == k), reverse=True)
            for k in range(1, deep + 1)]


def children(tree, d0, most):
    return [d for d in range(most, 0, -1) if tree[d] == d0]


def mixer(n_sp, n_tp, tok_ref, gain_in, wpool_ref, wgate_ref, wback_ref, out_ref,
          xs, ps, xg, w_p, w_g, w_b, pin, halo, boxm, inv_count, gate, sumsq, gain_ref,
          x_recv, p_recv, w_recv, halo_recv, peer_recv, swap_recv,
          x_send, p_send, w_send, peer_send, halo_send, swap_send, load_sem):
    layers = gain_ref.shape[0]
    tokens, feat = tok_ref.shape
    chan = wpool_ref.shape[2]
    rows_w = wpool_ref.shape[1]
    ct = tokens // CHUNKS
    half_tp = n_tp // 2
    n_z = n_sp // 2
    half_z = n_z // 2
    q_n = n_sp // n_tp
    sp = lax.axis_index("sp")
    tp = lax.axis_index("tp")

    def tp_at(d):
        return lax.rem(tp + (d + n_tp), n_tp)

    def sp_at(d):
        return lax.rem(sp + (2 * d + n_sp), n_sp)

    peer = sp + 1 - 2 * lax.rem(sp, 2)
    before = lax.rem(sp + n_sp - 1, n_sp)
    after = lax.rem(sp + 1, n_sp)
    quad = lax.rem(sp, q_n)
    swap_to = (q_n * lax.rem(tp + half_tp, n_tp) + quad, sp // q_n)
    swap_from = (q_n * tp + quad, lax.rem(sp // q_n + half_tp, n_tp))

    def jumps(trees, most):
        return sorted({d - tree[d] for tree in trees for d in range(1, most + 1)})

    barrier = pltpu.get_barrier_semaphore()
    greet = [{"sp": before}, {"sp": after}, {"sp": swap_from[0], "tp": swap_from[1]}]
    for j in jumps((STATE_TREE, POOLED_TREE), half_tp):
        greet += [{"tp": tp_at(j)}, {"tp": tp_at(-j)}]
    for j in jumps((PAIRS, FOURS), half_z):
        greet += [{"sp": sp_at(j)}, {"sp": sp_at(-j)}]
    for who in greet:
        pl.semaphore_signal(barrier, inc=1, device_id=who, device_id_type=MESH)

    def start(src, dst, send, recv, who):
        pltpu.make_async_remote_copy(src_ref=src, dst_ref=dst, send_sem=send, recv_sem=recv,
                                     device_id=who, device_id_type=MESH).start()

    def arrived(ref, sem, name="wait"):
        with scope(name):
            pltpu.make_async_copy(ref, ref, sem).wait()

    own_rows = pl.ds(pl.multiple_of(sp * rows_w, rows_w), rows_w)
    loads = [pltpu.make_async_copy(wpool_ref, w_p.at[:, own_rows], load_sem.at[0])]
    for c in range(CHUNKS):
        loads.append(pltpu.make_async_copy(tok_ref.at[pl.ds(c * ct, ct)], xs.at[0, c, tp], load_sem.at[1 + c]))
    loads.append(pltpu.make_async_copy(wgate_ref, w_g.at[:, own_rows], load_sem.at[1 + CHUNKS]))
    loads.append(pltpu.make_async_copy(gain_in, gain_ref, load_sem.at[2 + CHUNKS]))
    for load in loads:
        load.start()

    with scope("boxes"):
        window = lax.shift_left(2, (tp * chan) // (n_tp * chan // GROUPS))
        reach_w = window // 2
        grid_rows = tokens // GRID_W
        first = sp * grid_rows
        total = grid_rows * n_sp
        ti = lax.broadcasted_iota(jnp.int32, (tokens, tokens), 0)
        tj = lax.broadcasted_iota(jnp.int32, (tokens, tokens), 1)
        ri, ci = ti // GRID_W, ti % GRID_W
        cj = tj % GRID_W
        col_in = (cj >= ci - reach_w) & (cj < ci + reach_w)
        for k in range(3):
            rj = tj // GRID_W + (k - 1) * grid_rows
            inside = col_in & (rj >= ri - reach_w) & (rj < ri + reach_w)
            boxm[k] = jnp.where(inside, 1.0, 0.0).astype(BF16)
        tr = lax.broadcasted_iota(jnp.int32, (tokens, chan), 0)
        r_at, c_at = tr // GRID_W + first, tr % GRID_W
        r_n = jnp.minimum(r_at + reach_w, total) - jnp.maximum(r_at - reach_w, 0)
        c_n = jnp.minimum(c_at + reach_w, GRID_W) - jnp.maximum(c_at - reach_w, 0)
        inv_count[...] = 1.0 / (r_n * c_n).astype(F32)

        @pl.when(sp == 0)
        def _():
            for l in range(layers):
                halo[l, 0] = jnp.zeros((tokens, chan), BF16)

        @pl.when(sp == n_sp - 1)
        def _():
            for l in range(layers):
                halo[l, 1] = jnp.zeros((tokens, chan), BF16)

    with scope("barrier"):
        pl.semaphore_wait(barrier, len(greet))

    def reach(way, c):
        if half_tp * 2 == n_tp and (c % 2 == 0) != (way == 0):
            return half_tp - 1
        return half_tp

    def x_parts(buf):
        return (STATE_TREE, x_send, x_recv) if buf is xs else (POOLED_TREE, p_send, p_recv)

    def x_forward(buf, l, c, d0, way):
        tree, send, recv = x_parts(buf)
        step = 1 if way == 0 else -1
        block = buf.at[l, c, tp_at(-step * d0)]
        for d in children(tree, d0, reach(way, c)):
            start(block, block, send.at[l], recv.at[l, way, d - 1, c], {"tp": tp_at(step * (d - d0))})

    def x_wait(buf, l, c, d, way):
        recv = x_parts(buf)[2]
        step = 1 if way == 0 else -1
        arrived(buf.at[l, c, tp_at(-step * d)], recv.at[l, way, d - 1, c], f"x{'sp'[buf is ps]}{l}_d{d}_c{c}_w{way}")

    pieces = (w_p, w_g, w_b)

    def z_reach(way):
        return half_z if way == 0 else n_z - 1 - half_z

    def z_piece(kind, l, d):
        return pieces[kind].at[l, pl.ds(pl.multiple_of(sp_at(d) * rows_w, rows_w), rows_w)]

    def z_forward(kind, l, d0, way):
        step = 1 if way == 0 else -1
        piece = z_piece(kind, l, -step * d0)
        for d in children(weight_tree(kind, l), d0, z_reach(way)):
            start(piece, piece, w_send.at[kind, l], w_recv.at[kind, l, way, d - 1], {"sp": sp_at(step * (d - d0))})

    def z_peer(kind, l, d):
        piece = z_piece(kind, l, d)
        start(piece, piece, peer_send.at[kind, l], peer_recv.at[kind, l], {"sp": peer})

    def z_begin(kind, l):
        for way in (0, 1):
            z_forward(kind, l, 0, way)
        z_peer(kind, l, 0)

    def z_stage(kind, l, k):
        for d in stages(weight_tree(kind, l), half_z)[k - 1]:
            for way in (0, 1):
                step = 1 if way == 0 else -1
                if d <= z_reach(way):
                    arrived(z_piece(kind, l, -step * d), w_recv.at[kind, l, way, d - 1], f"z{'pgb'[kind]}{l}_d{d}_w{way}")
                    z_forward(kind, l, d, way)
                    z_peer(kind, l, -step * d)

    def z_end(kind, l):
        arrived(pieces[kind].at[l, pl.ds(0, n_z * rows_w)], peer_recv.at[kind, l], f"peer{'pgb'[kind]}{l}")

    def back_begin():
        arrived(w_b.at[:, own_rows], swap_recv, "swap")
        z_begin(BACK_W, 0)

    plan = {}

    def at(l, slot, *action):
        plan.setdefault((l, slot), []).append(action)

    at(0, "S2", z_stage, POOL_W, 0, 1)
    at(0, "S4", z_stage, POOL_W, 0, 2)
    at(0, "S4", z_end, POOL_W, 0)
    at(0, "S4", back_begin)
    at(0, "H", z_stage, GATE_W, 0, 1)
    at(0, "P1", z_stage, BACK_W, 0, 1)
    at(0, "P1", z_stage, GATE_W, 0, 2)
    at(0, "P1", z_end, GATE_W, 0)
    at(0, "P2", z_stage, BACK_W, 0, 2)
    at(0, "P2", z_end, BACK_W, 0)
    for l in range(1, layers):
        for kind in (POOL_W, GATE_W):
            at(l - 1, "H", z_begin, kind, l)
            at(l - 1, "P2", z_stage, kind, l, 1)
            at(l, "S1", z_stage, kind, l, 2)
            at(l, "S3", z_stage, kind, l, 3)
            at(l, "S4", z_stage, kind, l, 4)
            at(l, "S4", z_end, kind, l)
        at(l, "S1", z_begin, BACK_W, l)
        at(l, "S4", z_stage, BACK_W, l, 1)
        at(l, "P2", z_stage, BACK_W, l, 2)
        at(l, "P2", z_end, BACK_W, l)

    def slot(l, name):
        for action in plan.get((l, name), ()):
            action[0](*action[1:])

    def prep(l, c, j):
        block = xs[l, c, j].astype(F32)
        lanes = pl.ds(pl.multiple_of(j * feat, feat), feat)
        squares = block * block
        part = squares[:, 0:128]
        for k in range(1, feat // 128):
            part = part + squares[:, k * 128:(k + 1) * 128]
        sumsq[c * ct:(c + 1) * ct, :] += part
        xg[c * ct:(c + 1) * ct, lanes] = (block * gain_ref[l:l + 1, lanes]).astype(BF16)

    loads[0].wait()
    z_begin(POOL_W, 0)
    for c in range(CHUNKS):
        loads[1 + c].wait()
        for way in (0, 1):
            x_forward(xs, 0, c, 0, way)
    loads[1 + CHUNKS].wait()
    start(wback_ref, w_b.at[:, pl.ds(pl.multiple_of(swap_to[0] * rows_w, rows_w), rows_w)], swap_send, swap_recv,
          {"sp": swap_to[0], "tp": swap_to[1]})
    z_begin(GATE_W, 0)
    loads[2 + CHUNKS].wait()

    def x_gather(buf, l, name, each, last):
        deep = stages(x_parts(buf)[0], half_tp)
        for k, ds in enumerate(deep, 1):
            if k == len(deep) and last is not None:
                slot(l, f"{name}{k}")
            for c in range(CHUNKS):
                got = []
                for d in ds:
                    for way in (0, 1):
                        if d <= reach(way, c):
                            x_wait(buf, l, c, d, way)
                            x_forward(buf, l, c, d, way)
                            got.append(-d if way == 0 else d)
                if each is not None:
                    for d in got:
                        each(c, tp_at(d))
                if k == len(deep) and last is not None:
                    last(c)
            if k < len(deep) or last is None:
                slot(l, f"{name}{k}")

    for l in range(layers):
        sumsq[...] = jnp.zeros_like(sumsq)
        for c in range(CHUNKS):
            prep(l, c, tp)
        x_gather(xs, l, "S", functools.partial(prep, l), None)

        scale = lax.rsqrt(jnp.sum(sumsq[...], axis=1, keepdims=True) * (1.0 / (n_tp * feat)) + EPS)
        pool = jnp.dot(xg[...], w_p[l], preferred_element_type=F32)
        pin[l] = (pool * scale).astype(BF16)

        @pl.when(sp > 0)
        def _():
            start(pin.at[l], halo.at[l, 1], halo_send.at[l, 1], halo_recv.at[l, 1], {"sp": before})

        @pl.when(sp < n_sp - 1)
        def _():
            start(pin.at[l], halo.at[l, 0], halo_send.at[l, 0], halo_recv.at[l, 0], {"sp": after})

        def make_gate():
            rows_scale = lax.rsqrt(jnp.sum(sumsq[...], axis=1, keepdims=True) * (1.0 / (n_tp * feat)) + EPS)
            gate_acc = jnp.dot(xg[...], w_g[l], preferred_element_type=F32)
            gate[...] = jax.nn.sigmoid(gate_acc * rows_scale)

        slot(l, "H")
        if l > 0:
            make_gate()
        own_pool = pin[l]
        box = jnp.dot(boxm[1], own_pool, preferred_element_type=F32)

        @pl.when(sp > 0)
        def _():
            arrived(halo.at[l, 0], halo_recv.at[l, 0], f"halo{l}_0")

        @pl.when(sp < n_sp - 1)
        def _():
            arrived(halo.at[l, 1], halo_recv.at[l, 1], f"halo{l}_1")

        box = box + jnp.dot(boxm[0], halo[l, 0], preferred_element_type=F32)
        box = box + jnp.dot(boxm[2], halo[l, 1], preferred_element_type=F32)
        pooled = (box * inv_count[...] - own_pool.astype(F32)).astype(BF16)
        for c in range(CHUNKS):
            ps[l, c, tp] = pooled[c * ct:(c + 1) * ct]
            for way in (0, 1):
                x_forward(ps, l, c, 0, way)

        def finish(c):
            if l == 0 and c == 0:
                make_gate()
            branch = None
            for p in range(n_tp):
                term = lax.dot_general(ps[l, c, (p + half_tp) % n_tp], w_b[l, p * feat:(p + 1) * feat],
                                       (((1,), (1,)), ((), ())), preferred_element_type=F32)
                branch = term if branch is None else branch + term
            rows = slice(c * ct, (c + 1) * ct)
            new = (xs[l, c, tp].astype(F32) + gate[rows] * branch).astype(BF16)
            if l + 1 < layers:
                xs[l + 1, c, tp] = new
                for way in (0, 1):
                    x_forward(xs, l + 1, c, 0, way)
            else:
                out_ref[rows, :] = new

        x_gather(ps, l, "P", None, finish)

    arrived(wback_ref, swap_send)

    def drained(ref, rows, sem):
        while rows:
            now = min(rows, ref.shape[0])
            arrived(ref.at[pl.ds(0, now)], sem)
            rows -= now

    sent = {buf_i: sum(reach(way, c) for way in (0, 1) for c in range(CHUNKS)) for buf_i in (0, 1)}
    for l in range(layers):
        for buf, send in ((xs, x_send), (ps, p_send)):
            left = sent[0]
            c = 0
            while left:
                now = min(left, n_tp)
                arrived(buf.at[l, c % CHUNKS, pl.ds(0, now)], send.at[l])
                left -= now
                c += 1
        for kind in range(3):
            drained(pieces[kind].at[l], (z_reach(0) + z_reach(1)) * rows_w, w_send.at[kind, l])
            drained(pieces[kind].at[l], n_z * rows_w, peer_send.at[kind, l])

        @pl.when(sp > 0)
        def _():
            arrived(pin.at[l], halo_send.at[l, 1])

        @pl.when(sp < n_sp - 1)
        def _():
            arrived(pin.at[l], halo_send.at[l, 0])


def solution(mesh):
    n_sp, n_tp = mesh.shape["sp"], mesh.shape["tp"]

    def on_device(tokens_in, norm_gain, w_pool_in, w_gate, w_back):
        layers = norm_gain.shape[0]
        tokens, feat = tokens_in.shape
        rows_w, chan = w_pool_in.shape[1:]
        rows = n_sp * rows_w
        ct = tokens // CHUNKS
        half_tp = n_tp // 2
        half_z = n_sp // 4
        dma = pltpu.SemaphoreType.DMA
        return pl.pallas_call(
            functools.partial(mixer, n_sp, n_tp),
            out_shape=jax.ShapeDtypeStruct((tokens, feat), BF16),
            in_specs=[pl.BlockSpec(memory_space=pltpu.HBM)] * 5,
            out_specs=pl.BlockSpec(memory_space=pltpu.VMEM),
            scratch_shapes=[
                pltpu.VMEM((layers, CHUNKS, n_tp, ct, feat), BF16),
                pltpu.VMEM((layers, CHUNKS, n_tp, ct, chan), BF16),
                pltpu.VMEM((tokens, n_tp * feat), BF16),
                pltpu.VMEM((layers, rows, chan), BF16),
                pltpu.VMEM((layers, rows, feat), BF16),
                pltpu.VMEM((layers, rows, chan), BF16),
                pltpu.VMEM((layers, tokens, chan), BF16),
                pltpu.VMEM((layers, 2, tokens, chan), BF16),
                pltpu.VMEM((3, tokens, tokens), BF16),
                pltpu.VMEM((tokens, chan), F32),
                pltpu.VMEM((tokens, feat), F32),
                pltpu.VMEM((tokens, 128), F32),
                pltpu.VMEM(norm_gain.shape, F32),
                dma((layers, 2, half_tp, CHUNKS)),
                dma((layers, 2, half_tp, CHUNKS)),
                dma((3, layers, 2, half_z)),
                dma((layers, 2)),
                dma((3, layers)),
                dma,
                dma((layers,)),
                dma((layers,)),
                dma((3, layers)),
                dma((3, layers)),
                dma((layers, 2)),
                dma,
                dma((3 + CHUNKS,)),
            ],
            compiler_params=pltpu.CompilerParams(
                collective_id=0, has_side_effects=True, vmem_limit_bytes=67043328),
        )(tokens_in, norm_gain, w_pool_in, w_gate, jnp.swapaxes(w_back, 1, 2))

    return jax.shard_map(
        on_device,
        mesh=mesh,
        in_specs=(
            P(("grp", "sp"), "tp"),
            P(),
            P(None, "sp", "tp"),
            P(None, "sp", "tp"),
            P(None, "tp", "sp"),
        ),
        out_specs=P(("grp", "sp"), "tp"),
        check_vma=False,
    )
```

```python
import functools

import jax
import jax.numpy as jnp
from jax import lax
from jax.experimental import pallas as pl
from jax.experimental.pallas import tpu as pltpu
from jax.sharding import PartitionSpec as P

MESH = pl.DeviceIdType.MESH
F32 = jnp.float32
BF16 = jnp.bfloat16
GRID_W = 32
GROUPS = 4
EPS = 1e-6
CHUNKS = 2
scope = jax.named_scope

RING = {1: 0, 2: 1, 3: 2, 4: 3}
PAIRS = {1: 0, 2: 0, 3: 2, 4: 2, 5: 4, 6: 4, 7: 6, 8: 6}
FOURS = {1: 0, 2: 0, 3: 0, 4: 0, 5: 4, 6: 4, 7: 4, 8: 4}
STATE_TREE = RING
POOLED_TREE = PAIRS
POOL_W, GATE_W, BACK_W = 0, 1, 2


def weight_tree(kind, l):
    if l == 0:
        return FOURS
    return PAIRS


def depth(tree, d):
    return 0 if d == 0 else 1 + depth(tree, tree[d])


def stages(tree, most):
    deep = max(depth(tree, d) for d in range(1, most + 1))
    return [sorted((d for d in range(1, most + 1) if depth(tree, d) == k), reverse=True)
            for k in range(1, deep + 1)]


def children(tree, d0, most):
    return [d for d in range(most, 0, -1) if tree[d] == d0]


def mixer(n_sp, n_tp, tok_ref, gain_in, wpool_ref, wgate_ref, wback_ref, out_ref,
          xs, ps, xg, w_p, w_g, w_b, pin, halo, boxm, inv_count, gate, sumsq, gain_ref,
          x_recv, p_recv, w_recv, halo_recv, peer_recv, swap_recv,
          x_send, p_send, w_send, peer_send, halo_send, swap_send, load_sem):
    layers = gain_ref.shape[0]
    tokens, feat = tok_ref.shape
    chan = wpool_ref.shape[2]
    rows_w = wpool_ref.shape[1]
    ct = tokens // CHUNKS
    half_tp = n_tp // 2
    n_z = n_sp // 2
    half_z = n_z // 2
    q_n = n_sp // n_tp
    sp = lax.axis_index("sp")
    tp = lax.axis_index("tp")

    def tp_at(d):
        return lax.rem(tp + (d + n_tp), n_tp)

    def sp_at(d):
        return lax.rem(sp + (2 * d + n_sp), n_sp)

    peer = sp + 1 - 2 * lax.rem(sp, 2)
    before = lax.rem(sp + n_sp - 1, n_sp)
    after = lax.rem(sp + 1, n_sp)
    quad = lax.rem(sp, q_n)
    swap_to = (q_n * lax.rem(tp + half_tp, n_tp) + quad, sp // q_n)
    swap_from = (q_n * tp + quad, lax.rem(sp // q_n + half_tp, n_tp))

    def jumps(trees, most):
        return sorted({d - tree[d] for tree in trees for d in range(1, most + 1)})

    barrier = pltpu.get_barrier_semaphore()
    greet = [{"sp": before}, {"sp": after}, {"sp": swap_from[0], "tp": swap_from[1]}]
    for j in jumps((STATE_TREE, POOLED_TREE), half_tp):
        greet += [{"tp": tp_at(j)}, {"tp": tp_at(-j)}]
    for j in jumps((PAIRS, FOURS), half_z):
        greet += [{"sp": sp_at(j)}, {"sp": sp_at(-j)}]
    for who in greet:
        pl.semaphore_signal(barrier, inc=1, device_id=who, device_id_type=MESH)

    def start(src, dst, send, recv, who):
        pltpu.make_async_remote_copy(src_ref=src, dst_ref=dst, send_sem=send, recv_sem=recv,
                                     device_id=who, device_id_type=MESH).start()

    def arrived(ref, sem, name="wait"):
        with scope(name):
            pltpu.make_async_copy(ref, ref, sem).wait()

    own_rows = pl.ds(pl.multiple_of(sp * rows_w, rows_w), rows_w)
    loads = [pltpu.make_async_copy(wpool_ref, w_p.at[:, own_rows], load_sem.at[0])]
    for c in range(CHUNKS):
        loads.append(pltpu.make_async_copy(tok_ref.at[pl.ds(c * ct, ct)], xs.at[0, c, tp], load_sem.at[1 + c]))
    loads.append(pltpu.make_async_copy(wgate_ref, w_g.at[:, own_rows], load_sem.at[1 + CHUNKS]))
    loads.append(pltpu.make_async_copy(gain_in, gain_ref, load_sem.at[2 + CHUNKS]))
    for load in loads:
        load.start()

    with scope("boxes"):
        window = lax.shift_left(2, (tp * chan) // (n_tp * chan // GROUPS))
        reach_w = window // 2
        grid_rows = tokens // GRID_W
        first = sp * grid_rows
        total = grid_rows * n_sp
        ti = lax.broadcasted_iota(jnp.int32, (tokens, tokens), 0)
        tj = lax.broadcasted_iota(jnp.int32, (tokens, tokens), 1)
        ri, ci = ti // GRID_W, ti % GRID_W
        cj = tj % GRID_W
        col_in = (cj >= ci - reach_w) & (cj < ci + reach_w)
        for k in range(3):
            rj = tj // GRID_W + (k - 1) * grid_rows
            inside = col_in & (rj >= ri - reach_w) & (rj < ri + reach_w)
            boxm[k] = jnp.where(inside, 1.0, 0.0).astype(BF16)
        tr = lax.broadcasted_iota(jnp.int32, (tokens, chan), 0)
        r_at, c_at = tr // GRID_W + first, tr % GRID_W
        r_n = jnp.minimum(r_at + reach_w, total) - jnp.maximum(r_at - reach_w, 0)
        c_n = jnp.minimum(c_at + reach_w, GRID_W) - jnp.maximum(c_at - reach_w, 0)
        inv_count[...] = 1.0 / (r_n * c_n).astype(F32)

        @pl.when(sp == 0)
        def _():
            for l in range(layers):
                halo[l, 0] = jnp.zeros((tokens, chan), BF16)

        @pl.when(sp == n_sp - 1)
        def _():
            for l in range(layers):
                halo[l, 1] = jnp.zeros((tokens, chan), BF16)

    with scope("barrier"):
        pl.semaphore_wait(barrier, len(greet))

    def reach(way, c):
        if half_tp * 2 == n_tp and (c % 2 == 0) != (way == 0):
            return half_tp - 1
        return half_tp

    def x_parts(buf):
        return (STATE_TREE, x_send, x_recv) if buf is xs else (POOLED_TREE, p_send, p_recv)

    def x_forward(buf, l, c, d0, way):
        tree, send, recv = x_parts(buf)
        step = 1 if way == 0 else -1
        block = buf.at[l, c, tp_at(-step * d0)]
        for d in children(tree, d0, reach(way, c)):
            start(block, block, send.at[l], recv.at[l, way, d - 1, c], {"tp": tp_at(step * (d - d0))})

    def x_wait(buf, l, c, d, way):
        recv = x_parts(buf)[2]
        step = 1 if way == 0 else -1
        arrived(buf.at[l, c, tp_at(-step * d)], recv.at[l, way, d - 1, c], f"x{'sp'[buf is ps]}{l}_d{d}_c{c}_w{way}")

    pieces = (w_p, w_g, w_b)

    def z_reach(way):
        return half_z if way == 0 else n_z - 1 - half_z

    def z_piece(kind, l, d):
        return pieces[kind].at[l, pl.ds(pl.multiple_of(sp_at(d) * rows_w, rows_w), rows_w)]

    def z_forward(kind, l, d0, way):
        step = 1 if way == 0 else -1
        piece = z_piece(kind, l, -step * d0)
        for d in children(weight_tree(kind, l), d0, z_reach(way)):
            start(piece, piece, w_send.at[kind, l], w_recv.at[kind, l, way, d - 1], {"sp": sp_at(step * (d - d0))})

    def z_peer(kind, l, d):
        piece = z_piece(kind, l, d)
        start(piece, piece, peer_send.at[kind, l], peer_recv.at[kind, l], {"sp": peer})

    def z_begin(kind, l):
        for way in (0, 1):
            z_forward(kind, l, 0, way)
        z_peer(kind, l, 0)

    def z_stage(kind, l, k):
        for d in stages(weight_tree(kind, l), half_z)[k - 1]:
            for way in (0, 1):
                step = 1 if way == 0 else -1
                if d <= z_reach(way):
                    arrived(z_piece(kind, l, -step * d), w_recv.at[kind, l, way, d - 1], f"z{'pgb'[kind]}{l}_d{d}_w{way}")
                    z_forward(kind, l, d, way)
                    z_peer(kind, l, -step * d)

    def z_end(kind, l):
        arrived(pieces[kind].at[l, pl.ds(0, n_z * rows_w)], peer_recv.at[kind, l], f"peer{'pgb'[kind]}{l}")

    def back_begin():
        arrived(w_b.at[:, own_rows], swap_recv, "swap")
        z_begin(BACK_W, 0)

    plan = {}

    def at(l, slot, *action):
        plan.setdefault((l, slot), []).append(action)

    at(0, "S2", z_stage, POOL_W, 0, 1)
    at(0, "S3", back_begin)
    at(0, "S4", z_stage, POOL_W, 0, 2)
    at(0, "S4", z_end, POOL_W, 0)
    at(0, "I", z_stage, GATE_W, 0, 1)
    at(0, "I", z_stage, BACK_W, 0, 1)
    at(0, "P2", z_stage, GATE_W, 0, 2)
    at(0, "P2", z_stage, BACK_W, 0, 2)
    at(0, "P2", z_end, GATE_W, 0)
    at(0, "P2", z_end, BACK_W, 0)
    for l in range(1, layers):
        kinds = (POOL_W, GATE_W, BACK_W)
        for where, action, *more in (((l - 1, "I"), z_begin), ((l - 1, "P2"), z_stage, 1), ((l, "S1"), z_stage, 2),
                                     ((l, "S2"), z_stage, 3), ((l, "S3"), z_stage, 4), ((l, "S4"), z_end)):
            for kind in kinds:
                at(*where, action, kind, l, *more)

    def slot(l, name):
        for action in plan.get((l, name), ()):
            action[0](*action[1:])

    def prep(l, c, j):
        block = xs[l, c, j].astype(F32)
        lanes = pl.ds(pl.multiple_of(j * feat, feat), feat)
        squares = block * block
        part = squares[:, 0:128]
        for k in range(1, feat // 128):
            part = part + squares[:, k * 128:(k + 1) * 128]
        sumsq[c * ct:(c + 1) * ct, :] += part
        xg[c * ct:(c + 1) * ct, lanes] = (block * gain_ref[l:l + 1, lanes]).astype(BF16)

    loads[0].wait()
    z_begin(POOL_W, 0)
    for c in range(CHUNKS):
        loads[1 + c].wait()
        for way in (0, 1):
            x_forward(xs, 0, c, 0, way)
    loads[1 + CHUNKS].wait()
    start(wback_ref, w_b.at[:, pl.ds(pl.multiple_of(swap_to[0] * rows_w, rows_w), rows_w)], swap_send, swap_recv,
          {"sp": swap_to[0], "tp": swap_to[1]})
    z_begin(GATE_W, 0)
    loads[2 + CHUNKS].wait()

    def x_gather(buf, l, name, each, last):
        deep = stages(x_parts(buf)[0], half_tp)
        for k, ds in enumerate(deep, 1):
            if k == len(deep) and last is not None:
                slot(l, f"{name}{k}")
            for c in range(CHUNKS):
                got = []
                for d in ds:
                    for way in (0, 1):
                        if d <= reach(way, c):
                            x_wait(buf, l, c, d, way)
                            x_forward(buf, l, c, d, way)
                            got.append(-d if way == 0 else d)
                if each is not None:
                    for d in got:
                        each(c, tp_at(d))
                if k == len(deep) and last is not None:
                    last(c)
            if k < len(deep):
                slot(l, f"{name}{k}")
            elif last is None:
                for rest in range(k, 5):
                    slot(l, f"{name}{rest}")

    for l in range(layers):
        sumsq[...] = jnp.zeros_like(sumsq)
        for c in range(CHUNKS):
            prep(l, c, tp)
        x_gather(xs, l, "S", functools.partial(prep, l), None)

        scale = lax.rsqrt(jnp.sum(sumsq[...], axis=1, keepdims=True) * (1.0 / (n_tp * feat)) + EPS)
        pool = jnp.dot(xg[...], w_p[l], preferred_element_type=F32)
        pin[l] = (pool * scale).astype(BF16)

        @pl.when(sp > 0)
        def _():
            start(pin.at[l], halo.at[l, 1], halo_send.at[l, 1], halo_recv.at[l, 1], {"sp": before})

        @pl.when(sp < n_sp - 1)
        def _():
            start(pin.at[l], halo.at[l, 0], halo_send.at[l, 0], halo_recv.at[l, 0], {"sp": after})

        def make_gate():
            rows_scale = lax.rsqrt(jnp.sum(sumsq[...], axis=1, keepdims=True) * (1.0 / (n_tp * feat)) + EPS)
            gate_acc = jnp.dot(xg[...], w_g[l], preferred_element_type=F32)
            gate[...] = jax.nn.sigmoid(gate_acc * rows_scale)

        if l > 0:
            make_gate()
        own_pool = pin[l]
        box = jnp.dot(boxm[1], own_pool, preferred_element_type=F32)

        @pl.when(sp > 0)
        def _():
            arrived(halo.at[l, 0], halo_recv.at[l, 0], f"halo{l}_0")

        @pl.when(sp < n_sp - 1)
        def _():
            arrived(halo.at[l, 1], halo_recv.at[l, 1], f"halo{l}_1")

        box = box + jnp.dot(boxm[0], halo[l, 0], preferred_element_type=F32)
        box = box + jnp.dot(boxm[2], halo[l, 1], preferred_element_type=F32)
        pooled = (box * inv_count[...] - own_pool.astype(F32)).astype(BF16)
        for c in range(CHUNKS):
            ps[l, c, tp] = pooled[c * ct:(c + 1) * ct]
            for way in (0, 1):
                x_forward(ps, l, c, 0, way)
        slot(l, "I")

        def finish(c):
            if l == 0 and c == 0:
                make_gate()
            branch = None
            for p in range(n_tp):
                term = lax.dot_general(ps[l, c, (p + half_tp) % n_tp], w_b[l, p * feat:(p + 1) * feat],
                                       (((1,), (1,)), ((), ())), preferred_element_type=F32)
                branch = term if branch is None else branch + term
            rows = slice(c * ct, (c + 1) * ct)
            new = (xs[l, c, tp].astype(F32) + gate[rows] * branch).astype(BF16)
            if l + 1 < layers:
                xs[l + 1, c, tp] = new
                for way in (0, 1):
                    x_forward(xs, l + 1, c, 0, way)
            else:
                out_ref[rows, :] = new

        x_gather(ps, l, "P", None, finish)

    arrived(wback_ref, swap_send)

    def drained(ref, rows, sem):
        while rows:
            now = min(rows, ref.shape[0])
            arrived(ref.at[pl.ds(0, now)], sem)
            rows -= now

    sent = {buf_i: sum(reach(way, c) for way in (0, 1) for c in range(CHUNKS)) for buf_i in (0, 1)}
    for l in range(layers):
        for buf, send in ((xs, x_send), (ps, p_send)):
            left = sent[0]
            c = 0
            while left:
                now = min(left, n_tp)
                arrived(buf.at[l, c % CHUNKS, pl.ds(0, now)], send.at[l])
                left -= now
                c += 1
        for kind in range(3):
            drained(pieces[kind].at[l], (z_reach(0) + z_reach(1)) * rows_w, w_send.at[kind, l])
            drained(pieces[kind].at[l], n_z * rows_w, peer_send.at[kind, l])

        @pl.when(sp > 0)
        def _():
            arrived(pin.at[l], halo_send.at[l, 1])

        @pl.when(sp < n_sp - 1)
        def _():
            arrived(pin.at[l], halo_send.at[l, 0])


def solution(mesh):
    n_sp, n_tp = mesh.shape["sp"], mesh.shape["tp"]

    def on_device(tokens_in, norm_gain, w_pool_in, w_gate, w_back):
        layers = norm_gain.shape[0]
        tokens, feat = tokens_in.shape
        rows_w, chan = w_pool_in.shape[1:]
        rows = n_sp * rows_w
        ct = tokens // CHUNKS
        half_tp = n_tp // 2
        half_z = n_sp // 4
        dma = pltpu.SemaphoreType.DMA
        return pl.pallas_call(
            functools.partial(mixer, n_sp, n_tp),
            out_shape=jax.ShapeDtypeStruct((tokens, feat), BF16),
            in_specs=[pl.BlockSpec(memory_space=pltpu.HBM)] * 5,
            out_specs=pl.BlockSpec(memory_space=pltpu.VMEM),
            scratch_shapes=[
                pltpu.VMEM((layers, CHUNKS, n_tp, ct, feat), BF16),
                pltpu.VMEM((layers, CHUNKS, n_tp, ct, chan), BF16),
                pltpu.VMEM((tokens, n_tp * feat), BF16),
                pltpu.VMEM((layers, rows, chan), BF16),
                pltpu.VMEM((layers, rows, feat), BF16),
                pltpu.VMEM((layers, rows, chan), BF16),
                pltpu.VMEM((layers, tokens, chan), BF16),
                pltpu.VMEM((layers, 2, tokens, chan), BF16),
                pltpu.VMEM((3, tokens, tokens), BF16),
                pltpu.VMEM((tokens, chan), F32),
                pltpu.VMEM((tokens, feat), F32),
                pltpu.VMEM((tokens, 128), F32),
                pltpu.VMEM(norm_gain.shape, F32),
                dma((layers, 2, half_tp, CHUNKS)),
                dma((layers, 2, half_tp, CHUNKS)),
                dma((3, layers, 2, half_z)),
                dma((layers, 2)),
                dma((3, layers)),
                dma,
                dma((layers,)),
                dma((layers,)),
                dma((3, layers)),
                dma((3, layers)),
                dma((layers, 2)),
                dma,
                dma((3 + CHUNKS,)),
            ],
            compiler_params=pltpu.CompilerParams(
                collective_id=0, has_side_effects=True, vmem_limit_bytes=67043328),
        )(tokens_in, norm_gain, w_pool_in, w_gate, jnp.swapaxes(w_back, 1, 2))

    return jax.shard_map(
        on_device,
        mesh=mesh,
        in_specs=(
            P(("grp", "sp"), "tp"),
            P(),
            P(None, "sp", "tp"),
            P(None, "sp", "tp"),
            P(None, "tp", "sp"),
        ),
        out_specs=P(("grp", "sp"), "tp"),
        check_vma=False,
    )
```

```python
import functools

import jax
import jax.numpy as jnp
from jax import lax
from jax.experimental import pallas as pl
from jax.experimental.pallas import tpu as pltpu
from jax.sharding import PartitionSpec as P

MESH = pl.DeviceIdType.MESH
F32 = jnp.float32
BF16 = jnp.bfloat16
GRID_W = 32
GROUPS = 4
EPS = 1e-6
CHUNKS = 2
scope = jax.named_scope

RING = {1: 0, 2: 1, 3: 2, 4: 3}
PAIRS = {1: 0, 2: 0, 3: 2, 4: 2, 5: 4, 6: 4, 7: 6, 8: 6}
FOURS = {1: 0, 2: 0, 3: 0, 4: 0, 5: 4, 6: 4, 7: 4, 8: 4}
STATE_TREE = RING
POOLED_TREE = PAIRS
POOL_W, GATE_W, BACK_W = 0, 1, 2


def weight_tree(kind, l):
    if l == 0 and kind == POOL_W:
        return FOURS
    return PAIRS


def depth(tree, d):
    return 0 if d == 0 else 1 + depth(tree, tree[d])


def stages(tree, most):
    deep = max(depth(tree, d) for d in range(1, most + 1))
    return [sorted((d for d in range(1, most + 1) if depth(tree, d) == k), reverse=True)
            for k in range(1, deep + 1)]


def children(tree, d0, most):
    return [d for d in range(most, 0, -1) if tree[d] == d0]


def mixer(n_sp, n_tp, tok_ref, gain_in, wpool_ref, wgate_ref, wback_ref, out_ref,
          xs, ps, xg, w_p, w_g, w_b, pin, halo, boxm, inv_count, gate, sumsq, gain_ref, pool_acc,
          x_recv, p_recv, w_recv, halo_recv, peer_recv, swap_recv,
          x_send, p_send, w_send, peer_send, halo_send, swap_send, load_sem):
    layers = gain_ref.shape[0]
    tokens, feat = tok_ref.shape
    chan = wpool_ref.shape[2]
    rows_w = wpool_ref.shape[1]
    ct = tokens // CHUNKS
    half_tp = n_tp // 2
    n_z = n_sp // 2
    half_z = n_z // 2
    q_n = n_sp // n_tp
    sp = lax.axis_index("sp")
    tp = lax.axis_index("tp")

    def tp_at(d):
        return lax.rem(tp + (d + n_tp), n_tp)

    def sp_at(d):
        return lax.rem(sp + (2 * d + n_sp), n_sp)

    peer = sp + 1 - 2 * lax.rem(sp, 2)
    before = lax.rem(sp + n_sp - 1, n_sp)
    after = lax.rem(sp + 1, n_sp)
    quad = lax.rem(sp, q_n)
    swap_to = (q_n * lax.rem(tp + half_tp, n_tp) + quad, sp // q_n)
    swap_from = (q_n * tp + quad, lax.rem(sp // q_n + half_tp, n_tp))

    def jumps(trees, most):
        return sorted({d - tree[d] for tree in trees for d in range(1, most + 1)})

    barrier = pltpu.get_barrier_semaphore()
    greet = [{"sp": before}, {"sp": after}, {"sp": swap_from[0], "tp": swap_from[1]}]
    for j in jumps((STATE_TREE, POOLED_TREE), half_tp):
        greet += [{"tp": tp_at(j)}, {"tp": tp_at(-j)}]
    for j in jumps((PAIRS, FOURS), half_z):
        greet += [{"sp": sp_at(j)}, {"sp": sp_at(-j)}]
    for who in greet:
        pl.semaphore_signal(barrier, inc=1, device_id=who, device_id_type=MESH)

    def start(src, dst, send, recv, who):
        pltpu.make_async_remote_copy(src_ref=src, dst_ref=dst, send_sem=send, recv_sem=recv,
                                     device_id=who, device_id_type=MESH).start()

    def arrived(ref, sem, name="wait"):
        with scope(name):
            pltpu.make_async_copy(ref, ref, sem).wait()

    own_rows = pl.ds(pl.multiple_of(sp * rows_w, rows_w), rows_w)
    loads = [pltpu.make_async_copy(wpool_ref, w_p.at[:, own_rows], load_sem.at[0])]
    for c in range(CHUNKS):
        loads.append(pltpu.make_async_copy(tok_ref.at[pl.ds(c * ct, ct)], xs.at[0, c, tp], load_sem.at[1 + c]))
    loads.append(pltpu.make_async_copy(wgate_ref, w_g.at[:, own_rows], load_sem.at[1 + CHUNKS]))
    loads.append(pltpu.make_async_copy(gain_in, gain_ref, load_sem.at[2 + CHUNKS]))
    for load in loads:
        load.start()

    with scope("boxes"):
        window = lax.shift_left(2, (tp * chan) // (n_tp * chan // GROUPS))
        reach_w = window // 2
        grid_rows = tokens // GRID_W
        first = sp * grid_rows
        total = grid_rows * n_sp
        ti = lax.broadcasted_iota(jnp.int32, (tokens, tokens), 0)
        tj = lax.broadcasted_iota(jnp.int32, (tokens, tokens), 1)
        ri, ci = ti // GRID_W, ti % GRID_W
        cj = tj % GRID_W
        col_in = (cj >= ci - reach_w) & (cj < ci + reach_w)
        for k in range(3):
            rj = tj // GRID_W + (k - 1) * grid_rows
            inside = col_in & (rj >= ri - reach_w) & (rj < ri + reach_w)
            boxm[k] = jnp.where(inside, 1.0, 0.0).astype(BF16)
        tr = lax.broadcasted_iota(jnp.int32, (tokens, chan), 0)
        r_at, c_at = tr // GRID_W + first, tr % GRID_W
        r_n = jnp.minimum(r_at + reach_w, total) - jnp.maximum(r_at - reach_w, 0)
        c_n = jnp.minimum(c_at + reach_w, GRID_W) - jnp.maximum(c_at - reach_w, 0)
        inv_count[...] = 1.0 / (r_n * c_n).astype(F32)

        @pl.when(sp == 0)
        def _():
            for l in range(layers):
                halo[l, 0] = jnp.zeros((tokens, chan), BF16)

        @pl.when(sp == n_sp - 1)
        def _():
            for l in range(layers):
                halo[l, 1] = jnp.zeros((tokens, chan), BF16)

    with scope("barrier"):
        pl.semaphore_wait(barrier, len(greet))

    def reach(way, c):
        if half_tp * 2 == n_tp and (c % 2 == 0) != (way == 0):
            return half_tp - 1
        return half_tp

    def x_parts(buf):
        return (STATE_TREE, x_send, x_recv) if buf is xs else (POOLED_TREE, p_send, p_recv)

    def x_forward(buf, l, c, d0, way):
        tree, send, recv = x_parts(buf)
        step = 1 if way == 0 else -1
        block = buf.at[l, c, tp_at(-step * d0)]
        for d in children(tree, d0, reach(way, c)):
            start(block, block, send.at[l], recv.at[l, way, d - 1, c], {"tp": tp_at(step * (d - d0))})

    def x_wait(buf, l, c, d, way):
        recv = x_parts(buf)[2]
        step = 1 if way == 0 else -1
        arrived(buf.at[l, c, tp_at(-step * d)], recv.at[l, way, d - 1, c], f"x{'sp'[buf is ps]}{l}_d{d}_c{c}_w{way}")

    pieces = (w_p, w_g, w_b)

    def z_reach(way):
        return half_z if way == 0 else n_z - 1 - half_z

    def z_piece(kind, l, d):
        return pieces[kind].at[l, pl.ds(pl.multiple_of(sp_at(d) * rows_w, rows_w), rows_w)]

    def z_forward(kind, l, d0, way):
        step = 1 if way == 0 else -1
        piece = z_piece(kind, l, -step * d0)
        for d in children(weight_tree(kind, l), d0, z_reach(way)):
            start(piece, piece, w_send.at[kind, l], w_recv.at[kind, l, way, d - 1], {"sp": sp_at(step * (d - d0))})

    def z_peer(kind, l, d):
        piece = z_piece(kind, l, d)
        start(piece, piece, peer_send.at[kind, l], peer_recv.at[kind, l], {"sp": peer})

    def z_begin(kind, l):
        for way in (0, 1):
            z_forward(kind, l, 0, way)
        z_peer(kind, l, 0)

    def z_stage(kind, l, k):
        for d in stages(weight_tree(kind, l), half_z)[k - 1]:
            for way in (0, 1):
                step = 1 if way == 0 else -1
                if d <= z_reach(way):
                    arrived(z_piece(kind, l, -step * d), w_recv.at[kind, l, way, d - 1], f"z{'pgb'[kind]}{l}_d{d}_w{way}")
                    z_forward(kind, l, d, way)
                    z_peer(kind, l, -step * d)

    def z_end(kind, l):
        arrived(pieces[kind].at[l, pl.ds(0, n_z * rows_w)], peer_recv.at[kind, l], f"peer{'pgb'[kind]}{l}")

    def back_begin():
        arrived(w_b.at[0, own_rows], swap_recv.at[0], "swap")
        z_begin(BACK_W, 0)

    def swap_rest():
        arrived(w_b.at[pl.ds(1, layers - 1), own_rows], swap_recv.at[1], "swap")

    plan = {}

    def at(l, slot, *action):
        plan.setdefault((l, slot), []).append(action)

    at(0, "S2", z_stage, POOL_W, 0, 1)
    at(0, "S2", back_begin)
    at(0, "S2", z_stage, GATE_W, 0, 1)
    at(0, "S3", z_stage, GATE_W, 0, 2)
    at(0, "S3", z_stage, BACK_W, 0, 1)
    at(0, "S4", z_stage, POOL_W, 0, 2)
    at(0, "S4", z_stage, BACK_W, 0, 2)
    at(0, "S4", z_end, POOL_W, 0)
    at(0, "I", z_stage, GATE_W, 0, 3)
    at(0, "I", z_stage, BACK_W, 0, 3)
    at(0, "P1", z_stage, GATE_W, 0, 4)
    at(0, "P1", z_stage, BACK_W, 0, 4)
    at(0, "P2", z_end, GATE_W, 0)
    at(0, "P2", z_end, BACK_W, 0)
    at(0, "I", swap_rest)
    for l in range(1, layers):
        for kind in (POOL_W, GATE_W, BACK_W):
            at(l - 1, "I", z_begin, kind, l)
        for kind in (POOL_W, GATE_W, BACK_W):
            at(l - 1, "P1", z_stage, kind, l, 1)
        for kind in (POOL_W, GATE_W, BACK_W):
            at(l, "S1", z_stage, kind, l, 2)
        at(l, "S2", z_stage, POOL_W, l, 3)
        at(l, "S3", z_stage, POOL_W, l, 4)
        at(l, "S3", z_stage, GATE_W, l, 3)
        at(l, "S3", z_stage, BACK_W, l, 3)
        at(l, "S3", z_end, POOL_W, l)
        at(l, "I", z_stage, GATE_W, l, 4)
        at(l, "I", z_stage, BACK_W, l, 4)
        at(l, "P2", z_end, GATE_W, l)
        at(l, "P2", z_end, BACK_W, l)

    def slot(l, name):
        for action in plan.get((l, name), ()):
            action[0](*action[1:])

    def prep(l, c, j):
        block = xs[l, c, j].astype(F32)
        lanes = pl.ds(pl.multiple_of(j * feat, feat), feat)
        squares = block * block
        part = squares[:, 0:128]
        for k in range(1, feat // 128):
            part = part + squares[:, k * 128:(k + 1) * 128]
        sumsq[c * ct:(c + 1) * ct, :] += part
        xg[c * ct:(c + 1) * ct, lanes] = (block * gain_ref[l:l + 1, lanes]).astype(BF16)

    swap_rows = pl.ds(pl.multiple_of(swap_to[0] * rows_w, rows_w), rows_w)
    swap_who = {"sp": swap_to[0], "tp": swap_to[1]}
    start(wback_ref.at[0], w_b.at[0, swap_rows], swap_send.at[0], swap_recv.at[0], swap_who)
    for c in range(CHUNKS):
        loads[1 + c].wait()
        for way in (0, 1):
            x_forward(xs, 0, c, 0, way)
    loads[0].wait()
    z_begin(POOL_W, 0)
    loads[1 + CHUNKS].wait()
    z_begin(GATE_W, 0)
    rest = pl.ds(1, layers - 1)
    start(wback_ref.at[rest], w_b.at[rest, swap_rows], swap_send.at[1], swap_recv.at[1], swap_who)
    loads[2 + CHUNKS].wait()

    def pool_term(l, d):
        at_d = pl.ds(pl.multiple_of(tp_at(d) * feat, feat), feat)
        return jnp.dot(xg[:, at_d], w_p[l, at_d], preferred_element_type=F32)

    def ahead(l):
        if l > 0:
            total_here = pool_term(l, 0)
            for d in range(1, half_tp):
                total_here = total_here + pool_term(l, d) + pool_term(l, -d)
            pool_acc[...] = total_here

    def x_gather(buf, l, name, each, last):
        deep = stages(x_parts(buf)[0], half_tp)
        for k, ds in enumerate(deep, 1):
            if k == len(deep) and last is None:
                ahead(l)
            for c in range(CHUNKS):
                got = []
                for d in ds:
                    for way in (0, 1):
                        if d <= reach(way, c):
                            x_wait(buf, l, c, d, way)
                            x_forward(buf, l, c, d, way)
                            got.append(-d if way == 0 else d)
                if each is not None:
                    for d in got:
                        each(c, tp_at(d))
                if k == len(deep) and last is not None:
                    if c == 0:
                        slot(l, f"{name}{k}")
                    last(c)
            if k < len(deep):
                slot(l, f"{name}{k}")
            elif last is None:
                for rest in range(k, 5):
                    slot(l, f"{name}{rest}")

    for l in range(layers):
        sumsq[...] = jnp.zeros_like(sumsq)
        for c in range(CHUNKS):
            prep(l, c, tp)
        x_gather(xs, l, "S", functools.partial(prep, l), None)

        scale = lax.rsqrt(jnp.sum(sumsq[...], axis=1, keepdims=True) * (1.0 / (n_tp * feat)) + EPS)
        if l == 0:
            pool = jnp.dot(xg[...], w_p[l], preferred_element_type=F32)
        else:
            pool = pool_acc[...] + pool_term(l, half_tp)
        pin[l] = (pool * scale).astype(BF16)

        @pl.when(sp > 0)
        def _():
            start(pin.at[l], halo.at[l, 1], halo_send.at[l, 1], halo_recv.at[l, 1], {"sp": before})

        @pl.when(sp < n_sp - 1)
        def _():
            start(pin.at[l], halo.at[l, 0], halo_send.at[l, 0], halo_recv.at[l, 0], {"sp": after})

        def make_gate():
            rows_scale = lax.rsqrt(jnp.sum(sumsq[...], axis=1, keepdims=True) * (1.0 / (n_tp * feat)) + EPS)
            gate_acc = jnp.dot(xg[...], w_g[l], preferred_element_type=F32)
            gate[...] = jax.nn.sigmoid(gate_acc * rows_scale)

        own_pool = pin[l]
        box = jnp.dot(boxm[1], own_pool, preferred_element_type=F32)

        @pl.when(sp > 0)
        def _():
            arrived(halo.at[l, 0], halo_recv.at[l, 0], f"halo{l}_0")

        @pl.when(sp < n_sp - 1)
        def _():
            arrived(halo.at[l, 1], halo_recv.at[l, 1], f"halo{l}_1")

        box = box + jnp.dot(boxm[0], halo[l, 0], preferred_element_type=F32)
        box = box + jnp.dot(boxm[2], halo[l, 1], preferred_element_type=F32)
        pooled = (box * inv_count[...] - own_pool.astype(F32)).astype(BF16)
        for c in range(CHUNKS):
            ps[l, c, tp] = pooled[c * ct:(c + 1) * ct]
            for way in (0, 1):
                x_forward(ps, l, c, 0, way)
        slot(l, "I")

        def finish(c):
            if c == 0:
                make_gate()
            branch = None
            for p in range(n_tp):
                term = lax.dot_general(ps[l, c, (p + half_tp) % n_tp], w_b[l, p * feat:(p + 1) * feat],
                                       (((1,), (1,)), ((), ())), preferred_element_type=F32)
                branch = term if branch is None else branch + term
            rows = slice(c * ct, (c + 1) * ct)
            new = (xs[l, c, tp].astype(F32) + gate[rows] * branch).astype(BF16)
            if l + 1 < layers:
                xs[l + 1, c, tp] = new
                for way in (0, 1):
                    x_forward(xs, l + 1, c, 0, way)
            else:
                out_ref[rows, :] = new

        x_gather(ps, l, "P", None, finish)

    arrived(wback_ref.at[0], swap_send.at[0])
    arrived(wback_ref.at[rest], swap_send.at[1])

    def drained(ref, rows, sem):
        while rows:
            now = min(rows, ref.shape[0])
            arrived(ref.at[pl.ds(0, now)], sem)
            rows -= now

    sent = {buf_i: sum(reach(way, c) for way in (0, 1) for c in range(CHUNKS)) for buf_i in (0, 1)}
    for l in range(layers):
        for buf, send in ((xs, x_send), (ps, p_send)):
            left = sent[0]
            c = 0
            while left:
                now = min(left, n_tp)
                arrived(buf.at[l, c % CHUNKS, pl.ds(0, now)], send.at[l])
                left -= now
                c += 1
        for kind in range(3):
            drained(pieces[kind].at[l], (z_reach(0) + z_reach(1)) * rows_w, w_send.at[kind, l])
            drained(pieces[kind].at[l], n_z * rows_w, peer_send.at[kind, l])

        @pl.when(sp > 0)
        def _():
            arrived(pin.at[l], halo_send.at[l, 1])

        @pl.when(sp < n_sp - 1)
        def _():
            arrived(pin.at[l], halo_send.at[l, 0])


def solution(mesh):
    n_sp, n_tp = mesh.shape["sp"], mesh.shape["tp"]

    def on_device(tokens_in, norm_gain, w_pool_in, w_gate, w_back):
        layers = norm_gain.shape[0]
        tokens, feat = tokens_in.shape
        rows_w, chan = w_pool_in.shape[1:]
        rows = n_sp * rows_w
        ct = tokens // CHUNKS
        half_tp = n_tp // 2
        half_z = n_sp // 4
        dma = pltpu.SemaphoreType.DMA
        return pl.pallas_call(
            functools.partial(mixer, n_sp, n_tp),
            out_shape=pltpu.VMEM((tokens, feat), BF16),
            in_specs=[pl.BlockSpec(memory_space=pltpu.HBM)] * 5,
            out_specs=pl.BlockSpec(memory_space=pltpu.VMEM),
            scratch_shapes=[
                pltpu.VMEM((layers, CHUNKS, n_tp, ct, feat), BF16),
                pltpu.VMEM((layers, CHUNKS, n_tp, ct, chan), BF16),
                pltpu.VMEM((tokens, n_tp * feat), BF16),
                pltpu.VMEM((layers, rows, chan), BF16),
                pltpu.VMEM((layers, rows, feat), BF16),
                pltpu.VMEM((layers, rows, chan), BF16),
                pltpu.VMEM((layers, tokens, chan), BF16),
                pltpu.VMEM((layers, 2, tokens, chan), BF16),
                pltpu.VMEM((3, tokens, tokens), BF16),
                pltpu.VMEM((tokens, chan), F32),
                pltpu.VMEM((tokens, feat), F32),
                pltpu.VMEM((tokens, 128), F32),
                pltpu.VMEM(norm_gain.shape, F32),
                pltpu.VMEM((tokens, chan), F32),
                dma((layers, 2, half_tp, CHUNKS)),
                dma((layers, 2, half_tp, CHUNKS)),
                dma((3, layers, 2, half_z)),
                dma((layers, 2)),
                dma((3, layers)),
                dma((2,)),
                dma((layers,)),
                dma((layers,)),
                dma((3, layers)),
                dma((3, layers)),
                dma((layers, 2)),
                dma((2,)),
                dma((3 + CHUNKS,)),
            ],
            compiler_params=pltpu.CompilerParams(
                collective_id=0, has_side_effects=True, vmem_limit_bytes=66700000),
        )(tokens_in, norm_gain, w_pool_in, w_gate, jnp.swapaxes(w_back, 1, 2))

    return jax.shard_map(
        on_device,
        mesh=mesh,
        in_specs=(
            P(("grp", "sp"), "tp"),
            P(),
            P(None, "sp", "tp"),
            P(None, "sp", "tp"),
            P(None, "tp", "sp"),
        ),
        out_specs=P(("grp", "sp"), "tp"),
        check_vma=False,
    )
```

```python
import functools

import jax
import jax.numpy as jnp
from jax import lax
from jax.experimental import pallas as pl
from jax.experimental.pallas import tpu as pltpu
from jax.sharding import PartitionSpec as P

MESH = pl.DeviceIdType.MESH
F32 = jnp.float32
BF16 = jnp.bfloat16
GRID_W = 32
GROUPS = 4
EPS = 1e-6
CHUNKS = 4
scope = jax.named_scope

RING = {1: 0, 2: 1, 3: 2, 4: 3}
PAIRS = {1: 0, 2: 0, 3: 2, 4: 2, 5: 4, 6: 4, 7: 6, 8: 6}
FOURS = {1: 0, 2: 0, 3: 0, 4: 0, 5: 4, 6: 4, 7: 4, 8: 4}
MIXED = {1: 0, 2: 0, 3: 0, 4: 0, 5: 4, 6: 4, 7: 6, 8: 6}
STATE_TREE = RING
POOLED_TREE = PAIRS
POOL_W, GATE_W, BACK_W = 0, 1, 2


def weight_tree(kind, l):
    if kind == POOL_W:
        return FOURS
    return MIXED if kind == BACK_W and l == 0 else PAIRS


def depth(tree, d):
    return 0 if d == 0 else 1 + depth(tree, tree[d])


def stages(tree, most):
    deep = max(depth(tree, d) for d in range(1, most + 1))
    return [sorted((d for d in range(1, most + 1) if depth(tree, d) == k), reverse=True)
            for k in range(1, deep + 1)]


def children(tree, d0, most):
    return [d for d in range(most, 0, -1) if tree[d] == d0]


def mixer(n_sp, n_tp, tok_ref, gain_in, wpool_ref, wgate_ref, wback_ref, out_ref,
          xs, ps, xg, w_p, w_g, w_b, pin, halo, boxm, inv_count, gate, sumsq, gain_ref, pool_acc,
          x_recv, p_recv, w_recv, halo_recv, peer_recv, swap_recv, sent, load_sem):
    layers = gain_ref.shape[0]
    tokens, feat = tok_ref.shape
    chan = wpool_ref.shape[2]
    rows_w = wpool_ref.shape[1]
    ct = tokens // CHUNKS
    half_tp = n_tp // 2
    n_z = n_sp // 2
    half_z = n_z // 2
    q_n = n_sp // n_tp
    sp = lax.axis_index("sp")
    tp = lax.axis_index("tp")

    def tp_at(d):
        return lax.rem(tp + (d + n_tp), n_tp)

    def sp_at(d):
        return lax.rem(sp + (2 * d + n_sp), n_sp)

    peer = sp + 1 - 2 * lax.rem(sp, 2)
    before = lax.rem(sp + n_sp - 1, n_sp)
    after = lax.rem(sp + 1, n_sp)
    quad = lax.rem(sp, q_n)
    swap_to = (q_n * lax.rem(tp + half_tp, n_tp) + quad, sp // q_n)
    swap_from = (q_n * tp + quad, lax.rem(sp // q_n + half_tp, n_tp))

    def jumps(trees, most):
        return sorted({d - tree[d] for tree in trees for d in range(1, most + 1)})

    barrier = pltpu.get_barrier_semaphore()
    greet = [{"sp": before}, {"sp": after}, {"sp": swap_from[0], "tp": swap_from[1]}]
    for j in jumps((STATE_TREE, POOLED_TREE), half_tp):
        greet += [{"tp": tp_at(j)}, {"tp": tp_at(-j)}]
    for j in jumps((PAIRS, FOURS), half_z):
        greet += [{"sp": sp_at(j)}, {"sp": sp_at(-j)}]
    for who in greet:
        pl.semaphore_signal(barrier, inc=1, device_id=who, device_id_type=MESH)

    def start(src, dst, recv, who):
        pltpu.make_async_remote_copy(src_ref=src, dst_ref=dst, send_sem=sent, recv_sem=recv,
                                     device_id=who, device_id_type=MESH).start()

    def arrived(ref, sem, name="wait"):
        with scope(name):
            pltpu.make_async_copy(ref, ref, sem).wait()

    own_rows = pl.ds(pl.multiple_of(sp * rows_w, rows_w), rows_w)
    loads = [pltpu.make_async_copy(wpool_ref, w_p.at[:, own_rows], load_sem.at[0])]
    for c in range(CHUNKS):
        loads.append(pltpu.make_async_copy(tok_ref.at[pl.ds(c * ct, ct)], xs.at[0, c, tp], load_sem.at[1 + c]))
    loads.append(pltpu.make_async_copy(wgate_ref, w_g.at[:, own_rows], load_sem.at[1 + CHUNKS]))
    loads.append(pltpu.make_async_copy(gain_in, gain_ref, load_sem.at[2 + CHUNKS]))
    for load in loads:
        load.start()

    with scope("boxes"):
        window = lax.shift_left(2, (tp * chan) // (n_tp * chan // GROUPS))
        reach_w = window // 2
        grid_rows = tokens // GRID_W
        first = sp * grid_rows
        total = grid_rows * n_sp
        ti = lax.broadcasted_iota(jnp.int32, (tokens, tokens), 0)
        tj = lax.broadcasted_iota(jnp.int32, (tokens, tokens), 1)
        ri, ci = ti // GRID_W, ti % GRID_W
        cj = tj % GRID_W
        col_in = (cj >= ci - reach_w) & (cj < ci + reach_w)
        for k in range(3):
            rj = tj // GRID_W + (k - 1) * grid_rows
            inside = col_in & (rj >= ri - reach_w) & (rj < ri + reach_w)
            boxm[k] = jnp.where(inside, 1.0, 0.0).astype(BF16)
        tr = lax.broadcasted_iota(jnp.int32, (tokens, chan), 0)
        r_at, c_at = tr // GRID_W + first, tr % GRID_W
        r_n = jnp.minimum(r_at + reach_w, total) - jnp.maximum(r_at - reach_w, 0)
        c_n = jnp.minimum(c_at + reach_w, GRID_W) - jnp.maximum(c_at - reach_w, 0)
        inv_count[...] = 1.0 / (r_n * c_n).astype(F32)

        @pl.when(sp == 0)
        def _():
            for l in range(layers):
                halo[l, 0] = jnp.zeros((tokens, chan), BF16)

        @pl.when(sp == n_sp - 1)
        def _():
            for l in range(layers):
                halo[l, 1] = jnp.zeros((tokens, chan), BF16)

    with scope("barrier"):
        pl.semaphore_wait(barrier, len(greet))

    def reach(way, c):
        if half_tp * 2 == n_tp and (c % 2 == 0) != (way == 0):
            return half_tp - 1
        return half_tp

    def x_parts(buf):
        return (STATE_TREE, x_recv) if buf is xs else (POOLED_TREE, p_recv)

    def x_forward(buf, l, c, d0, way):
        tree, recv = x_parts(buf)
        step = 1 if way == 0 else -1
        block = buf.at[l, c, tp_at(-step * d0)]
        for d in children(tree, d0, reach(way, c)):
            start(block, block, recv.at[way, d - 1, c], {"tp": tp_at(step * (d - d0))})

    def x_wait(buf, l, c, d, way):
        recv = x_parts(buf)[1]
        step = 1 if way == 0 else -1
        arrived(buf.at[l, c, tp_at(-step * d)], recv.at[way, d - 1, c], f"x{'sp'[buf is ps]}{l}_d{d}_c{c}_w{way}")

    pieces = (w_p, w_g, w_b)

    def z_reach(way):
        return half_z if way == 0 else n_z - 1 - half_z

    def z_piece(kind, l, d):
        return pieces[kind].at[l, pl.ds(pl.multiple_of(sp_at(d) * rows_w, rows_w), rows_w)]

    def z_group(kind, l, d):
        tree = weight_tree(kind, l)
        if tree is FOURS and depth(tree, d) == 1 and not children(tree, d, half_z):
            return 2
        return depth(tree, d) - 1

    def z_forward(kind, l, d0, way):
        step = 1 if way == 0 else -1
        piece = z_piece(kind, l, -step * d0)
        for d in children(weight_tree(kind, l), d0, z_reach(way)):
            start(piece, piece, w_recv.at[kind, l, z_group(kind, l, d)], {"sp": sp_at(step * (d - d0))})

    def z_peer(kind, l, d):
        piece = z_piece(kind, l, d)
        start(piece, piece, peer_recv.at[kind, l], {"sp": peer})

    def z_begin(kind, l):
        for way in (0, 1):
            z_forward(kind, l, 0, way)
        z_peer(kind, l, 0)

    def z_stage(kind, l, k, forwarded=None):
        tree = weight_tree(kind, l)
        groups = {}
        for d in stages(tree, half_z)[k - 1]:
            if forwarded is None or forwarded == bool(children(tree, d, half_z)):
                groups.setdefault(z_group(kind, l, d), []).extend((d, way) for way in (0, 1) if d <= z_reach(way))
        for group, ones in groups.items():
            arrived(pieces[kind].at[l, pl.ds(0, len(ones) * rows_w)], w_recv.at[kind, l, group],
                    f"z{'pgb'[kind]}{l}_{k}_{group}")
            for d, way in ones:
                z_forward(kind, l, d, way)
            for d, way in ones:
                z_peer(kind, l, -d if way == 0 else d)

    def z_end(kind, l):
        arrived(pieces[kind].at[l, pl.ds(0, n_z * rows_w)], peer_recv.at[kind, l], f"peer{'pgb'[kind]}{l}")

    def back_begin():
        arrived(w_b.at[0, own_rows], swap_recv.at[0], "swap")
        z_begin(BACK_W, 0)

    def swap_rest():
        arrived(w_b.at[pl.ds(1, layers - 1), own_rows], swap_recv.at[1], "swap")

    def norm_scale():
        return lax.rsqrt(jnp.sum(sumsq[...], axis=1, keepdims=True) * (1.0 / (n_tp * feat)) + EPS)

    def make_gate(l):
        gate_acc = jnp.dot(xg[...], w_g[l], preferred_element_type=F32)
        gate[...] = jax.nn.sigmoid(gate_acc * norm_scale())

    plan = {}

    def at(l, slot, *action):
        plan.setdefault((l, slot), []).append(action)

    at(0, "S1", z_stage, POOL_W, 0, 1, True)
    at(0, "S2", z_stage, GATE_W, 0, 1)
    at(0, "S2", back_begin)
    at(0, "S3", z_stage, POOL_W, 0, 1, False)
    at(0, "S4", z_stage, POOL_W, 0, 2)
    at(0, "S4", z_end, POOL_W, 0)
    at(0, "H", z_stage, GATE_W, 0, 2)
    at(0, "H", z_stage, BACK_W, 0, 1)
    at(0, "I", z_stage, GATE_W, 0, 3)
    at(0, "I", z_stage, BACK_W, 0, 2)
    at(0, "I", swap_rest)
    at(0, "P1", z_stage, GATE_W, 0, 4)
    at(0, "P1", z_stage, BACK_W, 0, 3)
    for l in range(layers):
        if l > 0:
            for kind in (POOL_W, GATE_W, BACK_W):
                at(l - 1, "I", z_begin, kind, l)
            at(l - 1, "P2", z_stage, POOL_W, l, 1, True)
            at(l, "S0", z_stage, POOL_W, l, 1, False)
            at(l, "S2", z_stage, POOL_W, l, 2)
            at(l, "S3", z_end, POOL_W, l)
            for kind in (GATE_W, BACK_W):
                at(l, "S0", z_stage, kind, l, 1)
                at(l, "S1", z_stage, kind, l, 2)
                at(l, "S3", z_stage, kind, l, 3)
                at(l, "I", z_stage, kind, l, 4)
        gate_slot = "P1" if l > 0 else "P2"
        at(l, gate_slot, z_end, GATE_W, l)
        at(l, gate_slot, make_gate, l)
        at(l, "P2", z_end, BACK_W, l)

    def slot(l, name):
        for action in plan.get((l, name), ()):
            action[0](*action[1:])

    def prep(l, c, j):
        block = xs[l, c, j].astype(F32)
        lanes = pl.ds(pl.multiple_of(j * feat, feat), feat)
        squares = block * block
        part = squares[:, 0:128]
        for k in range(1, feat // 128):
            part = part + squares[:, k * 128:(k + 1) * 128]
        sumsq[c * ct:(c + 1) * ct, :] += part
        xg[c * ct:(c + 1) * ct, lanes] = (block * gain_ref[l:l + 1, lanes]).astype(BF16)

    swap_rows = pl.ds(pl.multiple_of(swap_to[0] * rows_w, rows_w), rows_w)
    swap_who = {"sp": swap_to[0], "tp": swap_to[1]}
    start(wback_ref.at[0], w_b.at[0, swap_rows], swap_recv.at[0], swap_who)
    for c in range(CHUNKS):
        loads[1 + c].wait()
        for way in (0, 1):
            x_forward(xs, 0, c, 0, way)
    loads[0].wait()
    z_begin(POOL_W, 0)
    loads[1 + CHUNKS].wait()
    z_begin(GATE_W, 0)
    rest = pl.ds(1, layers - 1)
    start(wback_ref.at[rest], w_b.at[rest, swap_rows], swap_recv.at[1], swap_who)
    loads[2 + CHUNKS].wait()

    def pool_term(l, d):
        at_d = pl.ds(pl.multiple_of(tp_at(d) * feat, feat), feat)
        return jnp.dot(xg[:, at_d], w_p[l, at_d], preferred_element_type=F32)

    def ahead(l):
        if l > 0:
            total_here = pool_term(l, 0)
            for d in range(1, half_tp):
                total_here = total_here + pool_term(l, d) + pool_term(l, -d)
            pool_acc[...] = total_here

    def x_gather(buf, l, name, each, last):
        deep = stages(x_parts(buf)[0], half_tp)
        for k, ds in enumerate(deep, 1):
            if k == len(deep) and last is None:
                ahead(l)
            for c in range(CHUNKS):
                got = []
                for d in ds:
                    for way in (0, 1):
                        if d <= reach(way, c):
                            x_wait(buf, l, c, d, way)
                            x_forward(buf, l, c, d, way)
                            got.append(-d if way == 0 else d)
                if each is not None:
                    for d in got:
                        each(c, tp_at(d))
                if k == len(deep) and last is not None:
                    if c == 0:
                        slot(l, f"{name}{k}")
                    last(c)
            if k < len(deep):
                slot(l, f"{name}{k}")
            elif last is None:
                for rest in range(k, 5):
                    slot(l, f"{name}{rest}")

    for l in range(layers):
        sumsq[...] = jnp.zeros_like(sumsq)
        for c in range(CHUNKS):
            prep(l, c, tp)
        slot(l, "S0")
        x_gather(xs, l, "S", functools.partial(prep, l), None)

        scale = norm_scale()
        if l == 0:
            pool = jnp.dot(xg[...], w_p[l], preferred_element_type=F32)
        else:
            pool = pool_acc[...] + pool_term(l, half_tp)
        pin[l] = (pool * scale).astype(BF16)

        @pl.when(sp > 0)
        def _():
            start(pin.at[l], halo.at[l, 1], halo_recv.at[l, 1], {"sp": before})

        @pl.when(sp < n_sp - 1)
        def _():
            start(pin.at[l], halo.at[l, 0], halo_recv.at[l, 0], {"sp": after})

        slot(l, "H")
        own_pool = pin[l]
        box = jnp.dot(boxm[1], own_pool, preferred_element_type=F32)

        @pl.when(sp > 0)
        def _():
            arrived(halo.at[l, 0], halo_recv.at[l, 0], f"halo{l}_0")

        @pl.when(sp < n_sp - 1)
        def _():
            arrived(halo.at[l, 1], halo_recv.at[l, 1], f"halo{l}_1")

        box = box + jnp.dot(boxm[0], halo[l, 0], preferred_element_type=F32)
        box = box + jnp.dot(boxm[2], halo[l, 1], preferred_element_type=F32)
        pooled = (box * inv_count[...] - own_pool.astype(F32)).astype(BF16)
        for c in range(CHUNKS):
            ps[l, c, tp] = pooled[c * ct:(c + 1) * ct]
            for way in (0, 1):
                x_forward(ps, l, c, 0, way)
        slot(l, "I")

        def finish(c):
            branch = None
            for p in range(n_tp):
                term = lax.dot_general(ps[l, c, (p + half_tp) % n_tp], w_b[l, p * feat:(p + 1) * feat],
                                       (((1,), (1,)), ((), ())), preferred_element_type=F32)
                branch = term if branch is None else branch + term
            rows = slice(c * ct, (c + 1) * ct)
            new = (xs[l, c, tp].astype(F32) + gate[rows] * branch).astype(BF16)
            if l + 1 < layers:
                xs[l + 1, c, tp] = new
                for way in (0, 1):
                    x_forward(xs, l + 1, c, 0, way)
            else:
                out_ref[rows, :] = new

        x_gather(ps, l, "P", None, finish)

    arrived(wback_ref, sent)
    rounds = sum(reach(way, c) for way in (0, 1) for c in range(CHUNKS))
    for l in range(layers):
        for buf in (xs, ps):
            for c in range(0, rounds, n_tp):
                arrived(buf.at[l, (c // n_tp) % CHUNKS, pl.ds(0, min(n_tp, rounds - c))], sent)
        for piece in pieces:
            arrived(piece.at[l, pl.ds(0, (n_z - 1) * rows_w)], sent)
            arrived(piece.at[l, pl.ds(0, n_z * rows_w)], sent)

        @pl.when(sp > 0)
        def _():
            arrived(pin.at[l], sent)

        @pl.when(sp < n_sp - 1)
        def _():
            arrived(pin.at[l], sent)


def solution(mesh):
    n_sp, n_tp = mesh.shape["sp"], mesh.shape["tp"]

    def on_device(tokens_in, norm_gain, w_pool_in, w_gate, w_back):
        layers = norm_gain.shape[0]
        tokens, feat = tokens_in.shape
        rows_w, chan = w_pool_in.shape[1:]
        rows = n_sp * rows_w
        ct = tokens // CHUNKS
        half_tp = n_tp // 2
        half_z = n_sp // 4
        dma = pltpu.SemaphoreType.DMA
        return pl.pallas_call(
            functools.partial(mixer, n_sp, n_tp),
            out_shape=pltpu.VMEM((tokens, feat), BF16),
            in_specs=[pl.BlockSpec(memory_space=pltpu.HBM)] * 5,
            out_specs=pl.BlockSpec(memory_space=pltpu.VMEM),
            scratch_shapes=[
                pltpu.VMEM((layers, CHUNKS, n_tp, ct, feat), BF16),
                pltpu.VMEM((layers, CHUNKS, n_tp, ct, chan), BF16),
                pltpu.VMEM((tokens, n_tp * feat), BF16),
                pltpu.VMEM((layers, rows, chan), BF16),
                pltpu.VMEM((layers, rows, feat), BF16),
                pltpu.VMEM((layers, rows, chan), BF16),
                pltpu.VMEM((layers, tokens, chan), BF16),
                pltpu.VMEM((layers, 2, tokens, chan), BF16),
                pltpu.VMEM((3, tokens, tokens), BF16),
                pltpu.VMEM((tokens, chan), F32),
                pltpu.VMEM((tokens, feat), F32),
                pltpu.VMEM((tokens, 128), F32),
                pltpu.VMEM(norm_gain.shape, F32),
                pltpu.VMEM((tokens, chan), F32),
                dma((2, half_tp, CHUNKS)),
                dma((2, half_tp, CHUNKS)),
                dma((3, layers, 4)),
                dma((layers, 2)),
                dma((3, layers)),
                dma((2,)),
                dma,
                dma((3 + CHUNKS,)),
            ],
            compiler_params=pltpu.CompilerParams(
                collective_id=0, has_side_effects=True, vmem_limit_bytes=66700000),
        )(tokens_in, norm_gain, w_pool_in, w_gate, jnp.swapaxes(w_back, 1, 2))

    return jax.shard_map(
        on_device,
        mesh=mesh,
        in_specs=(
            P(("grp", "sp"), "tp"),
            P(),
            P(None, "sp", "tp"),
            P(None, "sp", "tp"),
            P(None, "tp", "sp"),
        ),
        out_specs=P(("grp", "sp"), "tp"),
        check_vma=False,
    )
```

```python
import functools

import jax
import jax.numpy as jnp
from jax import lax
from jax.experimental import pallas as pl
from jax.experimental.pallas import tpu as pltpu
from jax.sharding import PartitionSpec as P

MESH = pl.DeviceIdType.MESH
F32 = jnp.float32
BF16 = jnp.bfloat16
GRID_W = 32
GROUPS = 4
EPS = 1e-6
CHUNKS = 4
POOLED_CHUNKS = 2
scope = jax.named_scope

RING = {1: 0, 2: 1, 3: 2, 4: 3}
PAIRS = {1: 0, 2: 0, 3: 2, 4: 2, 5: 4, 6: 4, 7: 6, 8: 6}
FOURS = {1: 0, 2: 0, 3: 0, 4: 0, 5: 4, 6: 4, 7: 4, 8: 4}
MIXED = {1: 0, 2: 0, 3: 0, 4: 0, 5: 4, 6: 4, 7: 6, 8: 6}
STATE_TREE = RING
POOLED_TREE = PAIRS
POOL_W, GATE_W, BACK_W = 0, 1, 2


def weight_tree(kind, l):
    if kind == POOL_W:
        return FOURS
    return MIXED if kind == BACK_W and l == 0 else PAIRS


def depth(tree, d):
    return 0 if d == 0 else 1 + depth(tree, tree[d])


def stages(tree, most):
    deep = max(depth(tree, d) for d in range(1, most + 1))
    return [sorted((d for d in range(1, most + 1) if depth(tree, d) == k), reverse=True)
            for k in range(1, deep + 1)]


def children(tree, d0, most):
    return [d for d in range(most, 0, -1) if tree[d] == d0]


def mixer(n_sp, n_tp, tok_ref, gain_in, wpool_ref, wgate_ref, wback_ref, out_ref,
          xs, ps, xg, w_p, w_g, w_b, pin, halo, boxm, inv_count, gate, sumsq, gain_ref, pool_acc,
          x_recv, p_recv, w_recv, halo_recv, peer_recv, swap_recv, sent, load_sem):
    layers = gain_ref.shape[0]
    tokens, feat = tok_ref.shape
    chan = wpool_ref.shape[2]
    rows_w = wpool_ref.shape[1]
    ct = tokens // CHUNKS
    pt = tokens // POOLED_CHUNKS
    half_tp = n_tp // 2
    n_z = n_sp // 2
    half_z = n_z // 2
    q_n = n_sp // n_tp
    sp = lax.axis_index("sp")
    tp = lax.axis_index("tp")

    def tp_at(d):
        return lax.rem(tp + (d + n_tp), n_tp)

    def sp_at(d):
        return lax.rem(sp + (2 * d + n_sp), n_sp)

    peer = sp + 1 - 2 * lax.rem(sp, 2)
    before = lax.rem(sp + n_sp - 1, n_sp)
    after = lax.rem(sp + 1, n_sp)
    quad = lax.rem(sp, q_n)
    swap_to = (q_n * lax.rem(tp + half_tp, n_tp) + quad, sp // q_n)
    swap_from = (q_n * tp + quad, lax.rem(sp // q_n + half_tp, n_tp))

    def jumps(trees, most):
        return sorted({d - tree[d] for tree in trees for d in range(1, most + 1)})

    barrier = pltpu.get_barrier_semaphore()
    greet = [{"sp": before}, {"sp": after}, {"sp": swap_from[0], "tp": swap_from[1]}]
    for j in jumps((STATE_TREE, POOLED_TREE), half_tp):
        greet += [{"tp": tp_at(j)}, {"tp": tp_at(-j)}]
    for j in jumps((PAIRS, FOURS), half_z):
        greet += [{"sp": sp_at(j)}, {"sp": sp_at(-j)}]
    for who in greet:
        pl.semaphore_signal(barrier, inc=1, device_id=who, device_id_type=MESH)

    def start(src, dst, recv, who):
        pltpu.make_async_remote_copy(src_ref=src, dst_ref=dst, send_sem=sent, recv_sem=recv,
                                     device_id=who, device_id_type=MESH).start()

    def arrived(ref, sem, name="wait"):
        with scope(name):
            pltpu.make_async_copy(ref, ref, sem).wait()

    own_rows = pl.ds(pl.multiple_of(sp * rows_w, rows_w), rows_w)
    loads = [pltpu.make_async_copy(wpool_ref, w_p.at[:, own_rows], load_sem.at[0])]
    for c in range(CHUNKS):
        loads.append(pltpu.make_async_copy(tok_ref.at[pl.ds(c * ct, ct)], xs.at[0, c, tp], load_sem.at[1 + c]))
    loads.append(pltpu.make_async_copy(wgate_ref, w_g.at[:, own_rows], load_sem.at[1 + CHUNKS]))
    loads.append(pltpu.make_async_copy(gain_in, gain_ref, load_sem.at[2 + CHUNKS]))
    for load in loads:
        load.start()

    with scope("barrier"):
        pl.semaphore_wait(barrier, len(greet))

    def reach(way, c):
        if half_tp * 2 == n_tp and (c % 2 == 0) != (way == 0):
            return half_tp - 1
        return half_tp

    def x_parts(buf):
        return (STATE_TREE, x_recv) if buf is xs else (POOLED_TREE, p_recv)

    def x_forward(buf, l, c, d0, way):
        tree, recv = x_parts(buf)
        step = 1 if way == 0 else -1
        block = buf.at[l, c, tp_at(-step * d0)]
        for d in children(tree, d0, reach(way, c)):
            start(block, block, recv.at[way, d - 1, c], {"tp": tp_at(step * (d - d0))})

    def x_wait(buf, l, c, d, way):
        recv = x_parts(buf)[1]
        step = 1 if way == 0 else -1
        arrived(buf.at[l, c, tp_at(-step * d)], recv.at[way, d - 1, c], f"x{'sp'[buf is ps]}{l}_d{d}_c{c}_w{way}")

    pieces = (w_p, w_g, w_b)

    def z_reach(way):
        return half_z if way == 0 else n_z - 1 - half_z

    def z_piece(kind, l, d):
        return pieces[kind].at[l, pl.ds(pl.multiple_of(sp_at(d) * rows_w, rows_w), rows_w)]

    def z_group(kind, l, d):
        tree = weight_tree(kind, l)
        if tree is FOURS and depth(tree, d) == 1 and not children(tree, d, half_z):
            return 2
        return depth(tree, d) - 1

    def z_forward(kind, l, d0, way):
        step = 1 if way == 0 else -1
        piece = z_piece(kind, l, -step * d0)
        for d in children(weight_tree(kind, l), d0, z_reach(way)):
            start(piece, piece, w_recv.at[kind, l, z_group(kind, l, d)], {"sp": sp_at(step * (d - d0))})

    def z_peer(kind, l, d):
        piece = z_piece(kind, l, d)
        start(piece, piece, peer_recv.at[kind, l], {"sp": peer})

    def z_begin(kind, l):
        for way in (0, 1):
            z_forward(kind, l, 0, way)
        z_peer(kind, l, 0)

    def z_stage(kind, l, k, forwarded=None):
        tree = weight_tree(kind, l)
        groups = {}
        for d in stages(tree, half_z)[k - 1]:
            if forwarded is None or forwarded == bool(children(tree, d, half_z)):
                groups.setdefault(z_group(kind, l, d), []).extend((d, way) for way in (0, 1) if d <= z_reach(way))
        for group, ones in groups.items():
            arrived(pieces[kind].at[l, pl.ds(0, len(ones) * rows_w)], w_recv.at[kind, l, group],
                    f"z{'pgb'[kind]}{l}_{k}_{group}")
            for d, way in ones:
                z_forward(kind, l, d, way)
            for d, way in ones:
                z_peer(kind, l, -d if way == 0 else d)

    def z_end(kind, l):
        arrived(pieces[kind].at[l, pl.ds(0, n_z * rows_w)], peer_recv.at[kind, l], f"peer{'pgb'[kind]}{l}")

    def back_begin():
        arrived(w_b.at[0, own_rows], swap_recv.at[0], "swap")
        z_begin(BACK_W, 0)

    def swap_rest():
        arrived(w_b.at[pl.ds(1, layers - 1), own_rows], swap_recv.at[1], "swap")

    def norm_scale(rows=slice(None)):
        return lax.rsqrt(jnp.sum(sumsq[rows], axis=1, keepdims=True) * (1.0 / (n_tp * feat)) + EPS)

    def make_gate(l):
        gate_acc = jnp.dot(xg[...], w_g[l], preferred_element_type=F32)
        gate[...] = jax.nn.sigmoid(gate_acc * norm_scale())

    plan = {}

    def at(l, slot, *action):
        plan.setdefault((l, slot), []).append(action)

    at(0, "S1", z_stage, POOL_W, 0, 1, True)
    at(0, "S2", z_stage, GATE_W, 0, 1)
    at(0, "S2", back_begin)
    at(0, "S3", z_stage, POOL_W, 0, 1, False)
    at(0, "S4", z_stage, POOL_W, 0, 2)
    at(0, "S4", z_end, POOL_W, 0)
    at(0, "H", z_stage, GATE_W, 0, 2)
    at(0, "H", z_stage, BACK_W, 0, 1)
    at(0, "I", z_stage, GATE_W, 0, 3)
    at(0, "I", z_stage, BACK_W, 0, 2)
    at(0, "I", swap_rest)
    at(0, "P1", z_stage, GATE_W, 0, 4)
    at(0, "P1", z_stage, BACK_W, 0, 3)
    for l in range(layers):
        if l > 0:
            for kind in (POOL_W, GATE_W, BACK_W):
                at(l - 1, "I", z_begin, kind, l)
            at(l - 1, "P2", z_stage, POOL_W, l, 1, True)
            at(l, "S0", z_stage, POOL_W, l, 1, False)
            at(l, "S2", z_stage, POOL_W, l, 2)
            at(l, "S3", z_end, POOL_W, l)
            for kind in (GATE_W, BACK_W):
                at(l, "S0", z_stage, kind, l, 1)
                at(l, "S1", z_stage, kind, l, 2)
                at(l, "S3", z_stage, kind, l, 3)
                at(l, "I", z_stage, kind, l, 4)
        gate_slot = "P1" if l > 0 else "P2"
        at(l, gate_slot, z_end, GATE_W, l)
        at(l, gate_slot, make_gate, l)
        at(l, "P2", z_end, BACK_W, l)

    def slot(l, name):
        for action in plan.get((l, name), ()):
            action[0](*action[1:])

    def prep(l, c, j):
        block = xs[l, c, j].astype(F32)
        lanes = pl.ds(pl.multiple_of(j * feat, feat), feat)
        squares = block * block
        part = squares[:, 0:128]
        for k in range(1, feat // 128):
            part = part + squares[:, k * 128:(k + 1) * 128]
        sumsq[c * ct:(c + 1) * ct, :] += part
        xg[c * ct:(c + 1) * ct, lanes] = (block * gain_ref[l:l + 1, lanes]).astype(BF16)

    swap_rows = pl.ds(pl.multiple_of(swap_to[0] * rows_w, rows_w), rows_w)
    swap_who = {"sp": swap_to[0], "tp": swap_to[1]}
    start(wback_ref.at[0], w_b.at[0, swap_rows], swap_recv.at[0], swap_who)
    for c in range(CHUNKS):
        loads[1 + c].wait()
        for way in (0, 1):
            x_forward(xs, 0, c, 0, way)
    loads[0].wait()
    z_begin(POOL_W, 0)
    loads[1 + CHUNKS].wait()
    z_begin(GATE_W, 0)
    rest = pl.ds(1, layers - 1)
    start(wback_ref.at[rest], w_b.at[rest, swap_rows], swap_recv.at[1], swap_who)
    loads[2 + CHUNKS].wait()

    with scope("boxes"):
        window = lax.shift_left(2, (tp * chan) // (n_tp * chan // GROUPS))
        reach_w = window // 2
        grid_rows = tokens // GRID_W
        first = sp * grid_rows
        total = grid_rows * n_sp
        ti = lax.broadcasted_iota(jnp.int32, (tokens, tokens), 0)
        tj = lax.broadcasted_iota(jnp.int32, (tokens, tokens), 1)
        ri, ci = ti // GRID_W, ti % GRID_W
        cj = tj % GRID_W
        col_in = (cj >= ci - reach_w) & (cj < ci + reach_w)
        for k in range(3):
            rj = tj // GRID_W + (k - 1) * grid_rows
            inside = col_in & (rj >= ri - reach_w) & (rj < ri + reach_w)
            boxm[k] = jnp.where(inside, 1.0, 0.0).astype(BF16)
        tr = lax.broadcasted_iota(jnp.int32, (tokens, chan), 0)
        r_at, c_at = tr // GRID_W + first, tr % GRID_W
        r_n = jnp.minimum(r_at + reach_w, total) - jnp.maximum(r_at - reach_w, 0)
        c_n = jnp.minimum(c_at + reach_w, GRID_W) - jnp.maximum(c_at - reach_w, 0)
        inv_count[...] = 1.0 / (r_n * c_n).astype(F32)

        @pl.when(sp == 0)
        def _():
            for l in range(layers):
                halo[l, 0] = jnp.zeros((tokens, chan), BF16)

        @pl.when(sp == n_sp - 1)
        def _():
            for l in range(layers):
                halo[l, 1] = jnp.zeros((tokens, chan), BF16)

    def pool_term(l, d):
        at_d = pl.ds(pl.multiple_of(tp_at(d) * feat, feat), feat)
        return jnp.dot(xg[:, at_d], w_p[l, at_d], preferred_element_type=F32)

    def ahead(l):
        if l > 0:
            total_here = pool_term(l, 0)
            for d in range(1, half_tp):
                total_here = total_here + pool_term(l, d) + pool_term(l, -d)
            pool_acc[...] = total_here

    def send_halo(l, rows):
        @pl.when(sp > 0)
        def _():
            start(pin.at[l, rows], halo.at[l, 1, rows], halo_recv.at[l, 1], {"sp": before})

        @pl.when(sp < n_sp - 1)
        def _():
            start(pin.at[l, rows], halo.at[l, 0, rows], halo_recv.at[l, 0], {"sp": after})

    def pool_chunk(l, c):
        rows = slice(c * ct, (c + 1) * ct)
        far = pl.ds(pl.multiple_of(tp_at(half_tp) * feat, feat), feat)
        term = jnp.dot(xg[rows, far], w_p[l, far], preferred_element_type=F32)
        pin[l, rows] = ((pool_acc[rows] + term) * norm_scale(rows)).astype(BF16)
        send_halo(l, pl.ds(c * ct, ct))

    def x_gather(buf, l, name, each, last):
        deep = stages(x_parts(buf)[0], half_tp)
        for k, ds in enumerate(deep, 1):
            if k == len(deep) and last is None:
                ahead(l)
            for c in range(buf.shape[1]):
                got = []
                for d in ds:
                    for way in (0, 1):
                        if d <= reach(way, c):
                            x_wait(buf, l, c, d, way)
                            x_forward(buf, l, c, d, way)
                            got.append(-d if way == 0 else d)
                if each is not None:
                    for d in got:
                        each(c, tp_at(d))
                if k == len(deep) and last is None and l > 0:
                    pool_chunk(l, c)
                if k == len(deep) and last is not None:
                    if c == 0:
                        slot(l, f"{name}{k}")
                    last(c)
            if k < len(deep):
                slot(l, f"{name}{k}")
            elif last is None:
                for rest in range(k, 5):
                    slot(l, f"{name}{rest}")

    for l in range(layers):
        sumsq[...] = jnp.zeros_like(sumsq)
        for c in range(CHUNKS):
            prep(l, c, tp)
        slot(l, "S0")
        x_gather(xs, l, "S", functools.partial(prep, l), None)

        if l == 0:
            pool = jnp.dot(xg[...], w_p[l], preferred_element_type=F32)
            pin[l] = (pool * norm_scale()).astype(BF16)
            send_halo(l, pl.ds(0, tokens))

        slot(l, "H")
        own_pool = pin[l]
        box = jnp.dot(boxm[1], own_pool, preferred_element_type=F32)

        @pl.when(sp > 0)
        def _():
            arrived(halo.at[l, 0], halo_recv.at[l, 0], f"halo{l}_0")

        @pl.when(sp < n_sp - 1)
        def _():
            arrived(halo.at[l, 1], halo_recv.at[l, 1], f"halo{l}_1")

        box = box + jnp.dot(boxm[0], halo[l, 0], preferred_element_type=F32)
        box = box + jnp.dot(boxm[2], halo[l, 1], preferred_element_type=F32)
        pooled = (box * inv_count[...] - own_pool.astype(F32)).astype(BF16)
        for c in range(POOLED_CHUNKS):
            ps[l, c, tp] = pooled[c * pt:(c + 1) * pt]
            for way in (0, 1):
                x_forward(ps, l, c, 0, way)
        slot(l, "I")

        def finish(c):
            branch = None
            for p in range(n_tp):
                term = lax.dot_general(ps[l, c, (p + half_tp) % n_tp], w_b[l, p * feat:(p + 1) * feat],
                                       (((1,), (1,)), ((), ())), preferred_element_type=F32)
                branch = term if branch is None else branch + term
            for i in range(pt // ct):
                k = c * (pt // ct) + i
                rows = slice(k * ct, (k + 1) * ct)
                new = (xs[l, k, tp].astype(F32) + gate[rows] * branch[i * ct:(i + 1) * ct]).astype(BF16)
                if l + 1 < layers:
                    xs[l + 1, k, tp] = new
                    for way in (0, 1):
                        x_forward(xs, l + 1, k, 0, way)
                else:
                    out_ref[rows, :] = new

        x_gather(ps, l, "P", None, finish)

    arrived(wback_ref, sent)
    for l in range(layers):
        for buf in (xs, ps):
            rounds = sum(reach(way, c) for way in (0, 1) for c in range(buf.shape[1]))
            for c in range(0, rounds, n_tp):
                arrived(buf.at[l, (c // n_tp) % buf.shape[1], pl.ds(0, min(n_tp, rounds - c))], sent)
        for piece in pieces:
            arrived(piece.at[l, pl.ds(0, (n_z - 1) * rows_w)], sent)
            arrived(piece.at[l, pl.ds(0, n_z * rows_w)], sent)

        @pl.when(sp > 0)
        def _():
            arrived(pin.at[l], sent)

        @pl.when(sp < n_sp - 1)
        def _():
            arrived(pin.at[l], sent)


def solution(mesh):
    n_sp, n_tp = mesh.shape["sp"], mesh.shape["tp"]

    def on_device(tokens_in, norm_gain, w_pool_in, w_gate, w_back):
        layers = norm_gain.shape[0]
        tokens, feat = tokens_in.shape
        rows_w, chan = w_pool_in.shape[1:]
        rows = n_sp * rows_w
        ct = tokens // CHUNKS
        half_tp = n_tp // 2
        half_z = n_sp // 4
        dma = pltpu.SemaphoreType.DMA
        return pl.pallas_call(
            functools.partial(mixer, n_sp, n_tp),
            out_shape=pltpu.VMEM((tokens, feat), BF16),
            in_specs=[pl.BlockSpec(memory_space=pltpu.HBM)] * 5,
            out_specs=pl.BlockSpec(memory_space=pltpu.VMEM),
            scratch_shapes=[
                pltpu.VMEM((layers, CHUNKS, n_tp, ct, feat), BF16),
                pltpu.VMEM((layers, POOLED_CHUNKS, n_tp, tokens // POOLED_CHUNKS, chan), BF16),
                pltpu.VMEM((tokens, n_tp * feat), BF16),
                pltpu.VMEM((layers, rows, chan), BF16),
                pltpu.VMEM((layers, rows, feat), BF16),
                pltpu.VMEM((layers, rows, chan), BF16),
                pltpu.VMEM((layers, tokens, chan), BF16),
                pltpu.VMEM((layers, 2, tokens, chan), BF16),
                pltpu.VMEM((3, tokens, tokens), BF16),
                pltpu.VMEM((tokens, chan), F32),
                pltpu.VMEM((tokens, feat), F32),
                pltpu.VMEM((tokens, 128), F32),
                pltpu.VMEM(norm_gain.shape, F32),
                pltpu.VMEM((tokens, chan), F32),
                dma((2, half_tp, CHUNKS)),
                dma((2, half_tp, POOLED_CHUNKS)),
                dma((3, layers, 4)),
                dma((layers, 2)),
                dma((3, layers)),
                dma((2,)),
                dma,
                dma((3 + CHUNKS,)),
            ],
            compiler_params=pltpu.CompilerParams(
                collective_id=0, has_side_effects=True, vmem_limit_bytes=66700000),
        )(tokens_in, norm_gain, w_pool_in, w_gate, jnp.swapaxes(w_back, 1, 2))

    return jax.shard_map(
        on_device,
        mesh=mesh,
        in_specs=(
            P(("grp", "sp"), "tp"),
            P(),
            P(None, "sp", "tp"),
            P(None, "sp", "tp"),
            P(None, "tp", "sp"),
        ),
        out_specs=P(("grp", "sp"), "tp"),
        check_vma=False,
    )
```

```python
import functools

import jax
import jax.numpy as jnp
from jax import lax
from jax.experimental import pallas as pl
from jax.experimental.pallas import tpu as pltpu
from jax.sharding import PartitionSpec as P

MESH = pl.DeviceIdType.MESH
F32 = jnp.float32
BF16 = jnp.bfloat16
GRID_W = 32
GROUPS = 4
EPS = 1e-6
CHUNKS = 4
POOLED_CHUNKS = 2
scope = jax.named_scope

RING = {1: 0, 2: 1, 3: 2, 4: 3}
PAIRS = {1: 0, 2: 0, 3: 2, 4: 2, 5: 4, 6: 4, 7: 6, 8: 6}
FOURS = {1: 0, 2: 0, 3: 0, 4: 0, 5: 4, 6: 4, 7: 4, 8: 4}
MIXED = {1: 0, 2: 0, 3: 0, 4: 0, 5: 4, 6: 4, 7: 6, 8: 6}
STATE_TREE = RING
POOLED_TREE = PAIRS
POOL_W, GATE_W, BACK_W = 0, 1, 2


def weight_tree(kind, l):
    if kind == POOL_W:
        return FOURS
    return MIXED if kind == BACK_W and l == 0 else PAIRS


def depth(tree, d):
    return 0 if d == 0 else 1 + depth(tree, tree[d])


def stages(tree, most):
    deep = max(depth(tree, d) for d in range(1, most + 1))
    return [sorted((d for d in range(1, most + 1) if depth(tree, d) == k), reverse=True)
            for k in range(1, deep + 1)]


def children(tree, d0, most):
    return [d for d in range(most, 0, -1) if tree[d] == d0]


def mixer(n_sp, n_tp, tok_ref, gain_in, wpool_ref, wgate_ref, wback_ref, out_ref,
          xs, ps, xg, w_p, w_g, w_b, pin, halo, boxm, inv_count, gate, sumsq, gain_ref, pool_acc,
          x_recv, p_recv, w_recv, halo_recv, peer_recv, swap_recv, sent, load_sem):
    layers = gain_ref.shape[0]
    tokens, feat = tok_ref.shape
    chan = wpool_ref.shape[2]
    rows_w = wpool_ref.shape[1]
    ct = tokens // CHUNKS
    pt = tokens // POOLED_CHUNKS
    half_tp = n_tp // 2
    n_z = n_sp // 2
    half_z = n_z // 2
    q_n = n_sp // n_tp
    sp = lax.axis_index("sp")
    tp = lax.axis_index("tp")

    def tp_at(d):
        return lax.rem(tp + (d + n_tp), n_tp)

    def sp_at(d):
        return lax.rem(sp + (2 * d + n_sp), n_sp)

    peer = sp + 1 - 2 * lax.rem(sp, 2)
    before = lax.rem(sp + n_sp - 1, n_sp)
    after = lax.rem(sp + 1, n_sp)
    quad = lax.rem(sp, q_n)
    swap_to = (q_n * lax.rem(tp + half_tp, n_tp) + quad, sp // q_n)
    swap_from = (q_n * tp + quad, lax.rem(sp // q_n + half_tp, n_tp))

    def jumps(trees, most):
        return sorted({d - tree[d] for tree in trees for d in range(1, most + 1)})

    barrier = pltpu.get_barrier_semaphore()
    greet = [{"sp": before}, {"sp": after}, {"sp": swap_from[0], "tp": swap_from[1]}]
    for j in jumps((STATE_TREE, POOLED_TREE), half_tp):
        greet += [{"tp": tp_at(j)}, {"tp": tp_at(-j)}]
    for j in jumps((PAIRS, FOURS), half_z):
        greet += [{"sp": sp_at(j)}, {"sp": sp_at(-j)}]
    for who in greet:
        pl.semaphore_signal(barrier, inc=1, device_id=who, device_id_type=MESH)

    def start(src, dst, recv, who):
        pltpu.make_async_remote_copy(src_ref=src, dst_ref=dst, send_sem=sent, recv_sem=recv,
                                     device_id=who, device_id_type=MESH).start()

    def arrived(ref, sem, name="wait"):
        with scope(name):
            pltpu.make_async_copy(ref, ref, sem).wait()

    own_rows = pl.ds(pl.multiple_of(sp * rows_w, rows_w), rows_w)
    loads = [pltpu.make_async_copy(wpool_ref, w_p.at[:, own_rows], load_sem.at[0])]
    for c in range(CHUNKS):
        loads.append(pltpu.make_async_copy(tok_ref.at[pl.ds(c * ct, ct)], xs.at[0, c, tp], load_sem.at[1 + c]))
    loads.append(pltpu.make_async_copy(wgate_ref, w_g.at[:, own_rows], load_sem.at[1 + CHUNKS]))
    loads.append(pltpu.make_async_copy(gain_in, gain_ref, load_sem.at[2 + CHUNKS]))
    for load in loads:
        load.start()

    with scope("barrier"):
        pl.semaphore_wait(barrier, len(greet))

    def reach(way, c):
        if half_tp * 2 == n_tp and (c % 2 == 0) != (way == 0):
            return half_tp - 1
        return half_tp

    def x_parts(buf):
        return (STATE_TREE, x_recv) if buf is xs else (POOLED_TREE, p_recv)

    def x_forward(buf, l, c, d0, way):
        tree, recv = x_parts(buf)
        step = 1 if way == 0 else -1
        block = buf.at[l, c, tp_at(-step * d0)]
        for d in children(tree, d0, reach(way, c)):
            start(block, block, recv.at[way, d - 1, c], {"tp": tp_at(step * (d - d0))})

    def x_wait(buf, l, c, d, way):
        recv = x_parts(buf)[1]
        step = 1 if way == 0 else -1
        arrived(buf.at[l, c, tp_at(-step * d)], recv.at[way, d - 1, c], f"x{'sp'[buf is ps]}{l}_d{d}_c{c}_w{way}")

    pieces = (w_p, w_g, w_b)

    def z_reach(way):
        return half_z if way == 0 else n_z - 1 - half_z

    def z_piece(kind, l, d):
        return pieces[kind].at[l, pl.ds(pl.multiple_of(sp_at(d) * rows_w, rows_w), rows_w)]

    def z_group(kind, l, d):
        tree = weight_tree(kind, l)
        if tree is FOURS and depth(tree, d) == 1 and not children(tree, d, half_z):
            return 2
        return depth(tree, d) - 1

    def z_forward(kind, l, d0, way):
        step = 1 if way == 0 else -1
        piece = z_piece(kind, l, -step * d0)
        for d in children(weight_tree(kind, l), d0, z_reach(way)):
            start(piece, piece, w_recv.at[kind, l, z_group(kind, l, d)], {"sp": sp_at(step * (d - d0))})

    def z_peer(kind, l, d):
        piece = z_piece(kind, l, d)
        start(piece, piece, peer_recv.at[kind, l], {"sp": peer})

    def z_begin(kind, l):
        for way in (0, 1):
            z_forward(kind, l, 0, way)
        z_peer(kind, l, 0)

    def z_stage(kind, l, k, forwarded=None):
        tree = weight_tree(kind, l)
        groups = {}
        for d in stages(tree, half_z)[k - 1]:
            if forwarded is None or forwarded == bool(children(tree, d, half_z)):
                groups.setdefault(z_group(kind, l, d), []).extend((d, way) for way in (0, 1) if d <= z_reach(way))
        for group, ones in groups.items():
            arrived(pieces[kind].at[l, pl.ds(0, len(ones) * rows_w)], w_recv.at[kind, l, group],
                    f"z{'pgb'[kind]}{l}_{k}_{group}")
            for d, way in ones:
                z_forward(kind, l, d, way)
            for d, way in ones:
                z_peer(kind, l, -d if way == 0 else d)

    def z_end(kind, l):
        arrived(pieces[kind].at[l, pl.ds(0, n_z * rows_w)], peer_recv.at[kind, l], f"peer{'pgb'[kind]}{l}")

    def back_begin():
        arrived(w_b.at[0, own_rows], swap_recv.at[0], "swap")
        z_begin(BACK_W, 0)

    def swap_rest():
        arrived(w_b.at[pl.ds(1, layers - 1), own_rows], swap_recv.at[1], "swap")

    def norm_scale(rows=slice(None)):
        return lax.rsqrt(jnp.sum(sumsq[rows], axis=1, keepdims=True) * (1.0 / (n_tp * feat)) + EPS)

    def make_gate(l):
        gate_acc = jnp.dot(xg[...], w_g[l], preferred_element_type=F32)
        gate[...] = jax.nn.sigmoid(gate_acc * norm_scale())

    plan = {}

    def at(l, slot, *action):
        plan.setdefault((l, slot), []).append(action)

    at(0, "S2", z_stage, POOL_W, 0, 1, True)
    at(0, "S3", z_stage, GATE_W, 0, 1)
    at(0, "S2", back_begin)
    at(0, "S3", z_stage, POOL_W, 0, 1, False)
    at(0, "S4", z_stage, POOL_W, 0, 2)
    at(0, "S4", z_end, POOL_W, 0)
    at(0, "H", z_stage, GATE_W, 0, 2)
    at(0, "H", z_stage, BACK_W, 0, 1)
    at(0, "I", z_stage, GATE_W, 0, 3)
    at(0, "I", z_stage, BACK_W, 0, 2)
    at(0, "I", swap_rest)
    at(0, "P1", z_stage, GATE_W, 0, 4)
    at(0, "P1", z_stage, BACK_W, 0, 3)
    for l in range(layers):
        if l > 0:
            for kind in (POOL_W, GATE_W, BACK_W):
                at(l - 1, "I", z_begin, kind, l)
            at(l - 1, "P2", z_stage, POOL_W, l, 1, True)
            at(l, "S0", z_stage, POOL_W, l, 1, False)
            at(l, "S2", z_stage, POOL_W, l, 2)
            at(l, "S3", z_end, POOL_W, l)
            for kind in (GATE_W, BACK_W):
                at(l, "S0", z_stage, kind, l, 1)
                at(l, "S1", z_stage, kind, l, 2)
                at(l, "S3", z_stage, kind, l, 3)
                at(l, "I", z_stage, kind, l, 4)
        gate_slot = "P1" if l > 0 else "P2"
        at(l, gate_slot, z_end, GATE_W, l)
        at(l, gate_slot, make_gate, l)
        at(l, "P2", z_end, BACK_W, l)

    def slot(l, name):
        for action in plan.get((l, name), ()):
            action[0](*action[1:])

    def prep(l, c, j):
        block = xs[l, c, j].astype(F32)
        lanes = pl.ds(pl.multiple_of(j * feat, feat), feat)
        squares = block * block
        part = squares[:, 0:128]
        for k in range(1, feat // 128):
            part = part + squares[:, k * 128:(k + 1) * 128]
        sumsq[c * ct:(c + 1) * ct, :] += part
        xg[c * ct:(c + 1) * ct, lanes] = (block * gain_ref[l:l + 1, lanes]).astype(BF16)

    swap_rows = pl.ds(pl.multiple_of(swap_to[0] * rows_w, rows_w), rows_w)
    swap_who = {"sp": swap_to[0], "tp": swap_to[1]}
    start(wback_ref.at[0], w_b.at[0, swap_rows], swap_recv.at[0], swap_who)
    for c in range(CHUNKS):
        loads[1 + c].wait()
        for way in (0, 1):
            x_forward(xs, 0, c, 0, way)
    loads[0].wait()
    z_begin(POOL_W, 0)
    loads[1 + CHUNKS].wait()
    z_begin(GATE_W, 0)
    rest = pl.ds(1, layers - 1)
    start(wback_ref.at[rest], w_b.at[rest, swap_rows], swap_recv.at[1], swap_who)
    loads[2 + CHUNKS].wait()

    with scope("boxes"):
        window = lax.shift_left(2, (tp * chan) // (n_tp * chan // GROUPS))
        reach_w = window // 2
        grid_rows = tokens // GRID_W
        first = sp * grid_rows
        total = grid_rows * n_sp
        ti = lax.broadcasted_iota(jnp.int32, (tokens, tokens), 0)
        tj = lax.broadcasted_iota(jnp.int32, (tokens, tokens), 1)
        ri, ci = ti // GRID_W, ti % GRID_W
        cj = tj % GRID_W
        col_in = (cj >= ci - reach_w) & (cj < ci + reach_w)
        for k in range(3):
            rj = tj // GRID_W + (k - 1) * grid_rows
            inside = col_in & (rj >= ri - reach_w) & (rj < ri + reach_w)
            boxm[k] = jnp.where(inside, 1.0, 0.0).astype(BF16)
        tr = lax.broadcasted_iota(jnp.int32, (tokens, chan), 0)
        r_at, c_at = tr // GRID_W + first, tr % GRID_W
        r_n = jnp.minimum(r_at + reach_w, total) - jnp.maximum(r_at - reach_w, 0)
        c_n = jnp.minimum(c_at + reach_w, GRID_W) - jnp.maximum(c_at - reach_w, 0)
        inv_count[...] = 1.0 / (r_n * c_n).astype(F32)

        @pl.when(sp == 0)
        def _():
            for l in range(layers):
                halo[l, 0] = jnp.zeros((tokens, chan), BF16)

        @pl.when(sp == n_sp - 1)
        def _():
            for l in range(layers):
                halo[l, 1] = jnp.zeros((tokens, chan), BF16)

    def pool_term(l, d):
        at_d = pl.ds(pl.multiple_of(tp_at(d) * feat, feat), feat)
        return jnp.dot(xg[:, at_d], w_p[l, at_d], preferred_element_type=F32)

    def ahead(l):
        if l > 0:
            total_here = pool_term(l, 0)
            for d in range(1, half_tp):
                total_here = total_here + pool_term(l, d) + pool_term(l, -d)
            pool_acc[...] = total_here

    def send_halo(l, rows):
        @pl.when(sp > 0)
        def _():
            start(pin.at[l, rows], halo.at[l, 1, rows], halo_recv.at[l, 1], {"sp": before})

        @pl.when(sp < n_sp - 1)
        def _():
            start(pin.at[l, rows], halo.at[l, 0, rows], halo_recv.at[l, 0], {"sp": after})

    def pool_chunk(l, c):
        rows = slice(c * ct, (c + 1) * ct)
        far = pl.ds(pl.multiple_of(tp_at(half_tp) * feat, feat), feat)
        term = jnp.dot(xg[rows, far], w_p[l, far], preferred_element_type=F32)
        pin[l, rows] = ((pool_acc[rows] + term) * norm_scale(rows)).astype(BF16)
        send_halo(l, pl.ds(c * ct, ct))

    def x_gather(buf, l, name, each, last):
        deep = stages(x_parts(buf)[0], half_tp)
        for k, ds in enumerate(deep, 1):
            if k == len(deep) and last is None:
                ahead(l)
            for c in range(buf.shape[1]):
                got = []
                for d in ds:
                    for way in (0, 1):
                        if d <= reach(way, c):
                            x_wait(buf, l, c, d, way)
                            x_forward(buf, l, c, d, way)
                            got.append(-d if way == 0 else d)
                if each is not None:
                    for d in got:
                        each(c, tp_at(d))
                if k == len(deep) and last is None and l > 0:
                    pool_chunk(l, c)
                if k == len(deep) and last is not None:
                    if c == 0:
                        slot(l, f"{name}{k}")
                    last(c)
            if k < len(deep):
                slot(l, f"{name}{k}")
            elif last is None:
                for rest in range(k, 5):
                    slot(l, f"{name}{rest}")

    for l in range(layers):
        sumsq[...] = jnp.zeros_like(sumsq)
        for c in range(CHUNKS):
            prep(l, c, tp)
        slot(l, "S0")
        x_gather(xs, l, "S", functools.partial(prep, l), None)

        if l == 0:
            pool = jnp.dot(xg[...], w_p[l], preferred_element_type=F32)
            pin[l] = (pool * norm_scale()).astype(BF16)
            send_halo(l, pl.ds(0, tokens))

        slot(l, "H")
        own_pool = pin[l]
        box = jnp.dot(boxm[1], own_pool, preferred_element_type=F32)

        @pl.when(sp > 0)
        def _():
            arrived(halo.at[l, 0], halo_recv.at[l, 0], f"halo{l}_0")

        @pl.when(sp < n_sp - 1)
        def _():
            arrived(halo.at[l, 1], halo_recv.at[l, 1], f"halo{l}_1")

        box = box + jnp.dot(boxm[0], halo[l, 0], preferred_element_type=F32)
        box = box + jnp.dot(boxm[2], halo[l, 1], preferred_element_type=F32)
        pooled = (box * inv_count[...] - own_pool.astype(F32)).astype(BF16)
        for c in range(POOLED_CHUNKS):
            ps[l, c, tp] = pooled[c * pt:(c + 1) * pt]
            for way in (0, 1):
                x_forward(ps, l, c, 0, way)
        slot(l, "I")

        def finish(c):
            branch = None
            for p in range(n_tp):
                term = lax.dot_general(ps[l, c, (p + half_tp) % n_tp], w_b[l, p * feat:(p + 1) * feat],
                                       (((1,), (1,)), ((), ())), preferred_element_type=F32)
                branch = term if branch is None else branch + term
            for i in range(pt // ct):
                k = c * (pt // ct) + i
                rows = slice(k * ct, (k + 1) * ct)
                new = (xs[l, k, tp].astype(F32) + gate[rows] * branch[i * ct:(i + 1) * ct]).astype(BF16)
                if l + 1 < layers:
                    xs[l + 1, k, tp] = new
                    for way in (0, 1):
                        x_forward(xs, l + 1, k, 0, way)
                else:
                    out_ref[rows, :] = new

        x_gather(ps, l, "P", None, finish)

    arrived(wback_ref, sent)
    for l in range(layers):
        for buf in (xs, ps):
            rounds = sum(reach(way, c) for way in (0, 1) for c in range(buf.shape[1]))
            for c in range(0, rounds, n_tp):
                arrived(buf.at[l, (c // n_tp) % buf.shape[1], pl.ds(0, min(n_tp, rounds - c))], sent)
        for piece in pieces:
            arrived(piece.at[l, pl.ds(0, (n_z - 1) * rows_w)], sent)
            arrived(piece.at[l, pl.ds(0, n_z * rows_w)], sent)

        @pl.when(sp > 0)
        def _():
            arrived(pin.at[l], sent)

        @pl.when(sp < n_sp - 1)
        def _():
            arrived(pin.at[l], sent)


def solution(mesh):
    n_sp, n_tp = mesh.shape["sp"], mesh.shape["tp"]

    def on_device(tokens_in, norm_gain, w_pool_in, w_gate, w_back):
        layers = norm_gain.shape[0]
        tokens, feat = tokens_in.shape
        rows_w, chan = w_pool_in.shape[1:]
        rows = n_sp * rows_w
        ct = tokens // CHUNKS
        half_tp = n_tp // 2
        half_z = n_sp // 4
        dma = pltpu.SemaphoreType.DMA
        return pl.pallas_call(
            functools.partial(mixer, n_sp, n_tp),
            out_shape=pltpu.VMEM((tokens, feat), BF16),
            in_specs=[pl.BlockSpec(memory_space=pltpu.HBM)] * 5,
            out_specs=pl.BlockSpec(memory_space=pltpu.VMEM),
            scratch_shapes=[
                pltpu.VMEM((layers, CHUNKS, n_tp, ct, feat), BF16),
                pltpu.VMEM((layers, POOLED_CHUNKS, n_tp, tokens // POOLED_CHUNKS, chan), BF16),
                pltpu.VMEM((tokens, n_tp * feat), BF16),
                pltpu.VMEM((layers, rows, chan), BF16),
                pltpu.VMEM((layers, rows, feat), BF16),
                pltpu.VMEM((layers, rows, chan), BF16),
                pltpu.VMEM((layers, tokens, chan), BF16),
                pltpu.VMEM((layers, 2, tokens, chan), BF16),
                pltpu.VMEM((3, tokens, tokens), BF16),
                pltpu.VMEM((tokens, chan), F32),
                pltpu.VMEM((tokens, feat), F32),
                pltpu.VMEM((tokens, 128), F32),
                pltpu.VMEM(norm_gain.shape, F32),
                pltpu.VMEM((tokens, chan), F32),
                dma((2, half_tp, CHUNKS)),
                dma((2, half_tp, POOLED_CHUNKS)),
                dma((3, layers, 4)),
                dma((layers, 2)),
                dma((3, layers)),
                dma((2,)),
                dma,
                dma((3 + CHUNKS,)),
            ],
            compiler_params=pltpu.CompilerParams(
                collective_id=0, has_side_effects=True, vmem_limit_bytes=66700000),
        )(tokens_in, norm_gain, w_pool_in, w_gate, jnp.swapaxes(w_back, 1, 2))

    return jax.shard_map(
        on_device,
        mesh=mesh,
        in_specs=(
            P(("grp", "sp"), "tp"),
            P(),
            P(None, "sp", "tp"),
            P(None, "sp", "tp"),
            P(None, "tp", "sp"),
        ),
        out_specs=P(("grp", "sp"), "tp"),
        check_vma=False,
    )
```
